128 devices in a mesh: sp: 16 (over z, y), dp: 8 (over x, core).
Axes of the slice: x: 4, y: 4, z: 4, core: 2. Of those that a mesh axis runs over, the one named last changes fastest.
Arguments:
- residual: bfloat16 [8, 2048, 2048], P('dp', 'sp'), may hold values from -6 to 6
- query: bfloat16 [8, 2048, 16, 128], P('dp', 'sp'), may hold values from -6 to 6
- key_value: bfloat16 [8, 2048, 16, 128], P('dp', 'sp'), may hold values from -6 to 6
- out_weight: bfloat16 [2048, 2048], P(None, 'dp'), may hold values from -0.125 to 0.125
- norm_gain: float32 [2048], replicated, may hold values from 0.1 to 1.9
- query_gain: float32 [64], replicated, may hold values from 1.5 to 4.5
- key_gain: float32 [64], replicated, may hold values from 1.5 to 4.5
- route_ids: int32 [8, 2048, 4], P('dp', 'sp'), may hold values from 0 to 127, all different within a row; in each aligned block of 128 rows (0 to 127, 128 to 255, ..., all dimensions but the last counted through in order) at most 6 rows name the same one
- route_weights: float32 [8, 2048, 4], P('dp', 'sp'), may hold values from 0.2 to 1
- shared_gate: bfloat16 [2048, 512], replicated, may hold values from -0.125 to 0.125
- shared_up: bfloat16 [2048, 512], replicated, may hold values from -0.125 to 0.125
- shared_down: bfloat16 [512, 2048], replicated, may hold values from -0.25 to 0.25
- expert_gate: bfloat16 [128, 2048, 512], P(('sp', 'dp')), may hold values from -0.125 to 0.125
- expert_up: bfloat16 [128, 2048, 512], P(('sp', 'dp')), may hold values from -0.125 to 0.125
- expert_down: bfloat16 [128, 512, 2048], P(('sp', 'dp')), may hold values from -0.25 to 0.25
Outputs:
- result: bfloat16 [8, 2048, 2048], P('dp', 'sp')
The draws below stay inside these ranges and needn't reach their ends.
Inputs may be any that keep to these rules, and one draw needn't show every extreme that they name: `route_ids`: each row names 4 different experts. Among the rows of one device no expert is named more than 6 times, a bound that some block reaches.
All inputs are finite; a program needn't handle non-finite values.
Results may differ from the reference program's by a relative error of at most 0.014.
The reference program's roundings to bfloat16 on the way count: a program that leaves them out, or rounds other values in their place, can miss the bound.
Values may be sent and summed in bfloat16 or wider, within the bound.
A program may use at most 128 MiB of HBM per device.

```python
import math
import jax
import jax.numpy as jnp
import numpy as np
from jax import lax

D = 2048
HD = 64
Q_HEADS = 32
KV_HEADS = 16
REP = 2
GRID_W = 64
EFF = 512
SFF = 512
EXPERTS = 128
TOP_K = 4
TOK_DEV = 128
LEN = 2048
SEQS = 8
CAP = 6
N_SP = 16
N_DP = 8


def key_base_draw(key):
    drawn = jax.random.normal(jax.random.fold_in(key, 11), (SEQS, LEN, KV_HEADS, HD), jnp.float32)
    return jnp.clip(drawn, -6.0, 6.0)


def draw_query(key, part):
    drawn = jax.random.normal(jax.random.fold_in(key, 21), (SEQS, LEN, KV_HEADS, REP * HD), jnp.float32)
    drawn = jnp.clip(drawn, -6.0, 6.0)
    return drawn.astype(jnp.bfloat16)


def draw_key_value(key, part):
    key_base = key_base_draw(key)
    values = jax.random.normal(jax.random.fold_in(key, 12), (SEQS, LEN, KV_HEADS, HD), jnp.float32)
    values = jnp.clip(values, -6.0, 6.0)
    return jnp.concatenate([key_base, values], axis=-1).astype(jnp.bfloat16)


def gain_draw(key, salt):
    spread = jax.random.uniform(jax.random.fold_in(key, salt), (HD,), jnp.float32, jnp.log(1.5), jnp.log(3.0))
    return jnp.exp(spread)


def draw_query_gain(key, part):
    return gain_draw(key, 31)


def draw_key_gain(key, part):
    return gain_draw(key, 32)


def level_of(stream_key, extent, cuts, smallest, high):
    factor_of, own = 1.0, jax.random.fold_in(stream_key, 6)
    for axis_at, shards_of in cuts:
        draws = jnp.exp(jax.random.uniform(jax.random.fold_in(own, axis_at), (shards_of,), jnp.float32, smallest / len(cuts), high / len(cuts)))
        factor_of = factor_of * jnp.repeat(draws, extent[axis_at] // shards_of).reshape([-1 if axis == axis_at else 1 for axis in range(len(extent))])
    return factor_of


def routed_block(rng, own, number, rows, amount, top, bound, lean):
    order = jax.random.permutation(rng, amount)
    crowded, usual = load_shares(amount, rows * top, bound, lean, True), load_shares(amount, rows * top, bound, lean, False)
    places = jnp.arange(amount)

    def named(lengths, turn):
        used = int((lengths > 0).sum())
        fixed = max(1, used // 4)
        moved = fixed + (places - fixed + turn * (used - fixed)) % max(1, amount - fixed)
        return jnp.zeros((amount,), jnp.int32).at[order[jnp.where(places < fixed, places, moved)]].set(jnp.asarray(lengths, jnp.int32))

    lengths = jnp.where(number % 4 == 0, named(crowded, number // 4), named(usual, number - number // 4 - 1))
    mixed = jax.random.permutation(jax.random.fold_in(own, 3), amount)
    donor, receiver = mixed[0:amount // 2 * 2:2], mixed[1:amount // 2 * 2:2]
    margin = jnp.minimum(lengths[donor] - 1, bound - lengths[receiver]) // 2
    margin = jnp.where((donor == order[0]) | (receiver == order[0]) | (lengths[receiver] == 0), 0, jnp.maximum(margin, 0))
    moved = jax.random.randint(jax.random.fold_in(own, 4), (amount // 2,), 0, 1 << 20) % (margin + 1)
    lengths = lengths.at[donor].add(-moved).at[receiver].add(moved)
    labels = jnp.searchsorted(jnp.cumsum(lengths), jnp.arange(rows * top), side="right").astype(jnp.int32)
    listing = labels.reshape(top, rows).T
    listing = listing[jax.random.permutation(jax.random.fold_in(own, 1), rows)]
    turn = jax.random.randint(jax.random.fold_in(own, 2), (rows, 1), 0, top)
    return jnp.take_along_axis(listing, (jnp.arange(top)[None, :] + turn) % top, axis=1)


def load_shares(count, total, limit, skew, full):
    loads = [(1 << 20) // math.isqrt(standing ** skew) + 1 for standing in range(1, count + 1)]
    largest = limit if full else min(limit, max(-(-total // count), total * loads[0] // sum(loads)))
    least = 1 if total - largest >= count - 1 else 0
    given, rest = [largest] + [least] * (count - 1), total - largest - least * (count - 1)
    while rest > 0:
        movable = [i for i in range(1, count) if given[i] < largest] or [i for i in range(1, count) if given[i] < limit]
        pool, left = sum([loads[i] for i in movable]), rest
        for i in movable:
            more = min(limit - given[i], max(1, left * loads[i] // pool), rest)
            given[i] = given[i] + more
            rest = rest - more
    return np.array(given)


def normal_values(rng, dims, scale, limit, cuts=(), held_as=jnp.bfloat16):
    entries = jax.random.normal(rng, dims, jnp.float32) * scale
    if len(cuts) > 0:
        entries = level_of(rng, dims, cuts, -0.22, 0.18) * entries
    return jnp.clip(entries, min=-limit, max=limit).astype(held_as)


def setup_inputs(seed: int = 0) -> dict:
    splits = jax.random.split(jax.random.key(seed), 16)
    residual = normal_values(splits[0], (SEQS, LEN, D), 1.0, 6.0, ((0, 8), (1, 16)))
    query = draw_query(jax.random.fold_in(splits[15], 71), 0)
    key_value = draw_key_value(jax.random.fold_in(splits[15], 71), 0)
    out_weight = normal_values(splits[3], (Q_HEADS * HD, D), (Q_HEADS * HD) ** -0.5, 0.125, ((1, 8),))
    norm_gain = jnp.clip(1.0 + 0.18 * jax.random.normal(splits[4], (D,), jnp.float32), 0.1, 1.9)
    query_gain = draw_query_gain(jax.random.fold_in(splits[15], 71), 0)
    key_gain = draw_key_gain(jax.random.fold_in(splits[15], 71), 0)
    route_ids_keys = jax.random.split(jax.random.fold_in(splits[7], 1), SEQS * LEN // TOK_DEV)
    route_ids_turns = jax.random.permutation(jax.random.fold_in(splits[7], 3), SEQS * LEN // TOK_DEV)
    route_ids = jax.vmap(lambda own, number: routed_block(jax.random.fold_in(splits[7], 2), own, number, TOK_DEV, EXPERTS, TOP_K, CAP, 2))(route_ids_keys, route_ids_turns).reshape((SEQS, LEN, TOP_K))
    route_weights = jnp.clip(jnp.exp(math.log(1.0) - 1.609438 * jax.random.uniform(splits[8], (SEQS, LEN, TOP_K), jnp.float32) ** level_of(splits[8], (SEQS, LEN, TOP_K), ((0, 8), (1, 16)), -0.2, 0.2)), 0.2, 1.0)
    shared_gate = normal_values(splits[9], (D, SFF), D ** -0.5, 0.125)
    shared_up = normal_values(splits[10], (D, SFF), D ** -0.5, 0.125)
    shared_down = normal_values(splits[11], (SFF, D), SFF ** -0.5, 0.25)
    expert_gate = normal_values(splits[12], (EXPERTS, D, EFF), D ** -0.5, 0.125, ((0, 128),))
    expert_up = normal_values(splits[13], (EXPERTS, D, EFF), D ** -0.5, 0.125, ((0, 128),))
    expert_down = normal_values(splits[14], (EXPERTS, EFF, D), EFF ** -0.5, 0.25, ((0, 128),))
    return {"residual": residual, "query": query, "key_value": key_value, "out_weight": out_weight, "norm_gain": norm_gain, "query_gain": query_gain, "key_gain": key_gain, "route_ids": route_ids, "route_weights": route_weights, "shared_gate": shared_gate, "shared_up": shared_up, "shared_down": shared_down, "expert_gate": expert_gate, "expert_up": expert_up, "expert_down": expert_down}


norm_eps = 1e-06
rope_theta = 10000.0
routed_scale = 2.5

def rotate_half(values, position, half_width):
    inverse_freq = rope_theta ** (-jnp.arange(0, half_width, 2, dtype=jnp.float32) / half_width)
    angles = position.astype(jnp.float32)[:, None] * inverse_freq[None, :]
    angles = jnp.concatenate([angles, angles], axis=-1)
    cosine = jnp.cos(angles)[:, None, :]
    sine_part = jnp.sin(angles)[:, None, :]
    first_half, second = jnp.split(values, 2, axis=-1)
    turned = jnp.concatenate([-second, first_half], axis=-1)
    return values * cosine + turned * sine_part

def prepare(values, gain_vector, grid_row, grid_col):
    head_dim = values.shape[-1]
    floats = values.astype(jnp.float32)
    normed = floats * lax.rsqrt(lax.optimization_barrier(jnp.mean(floats * floats, axis=-1, keepdims=True)) + norm_eps)
    normed = normed * gain_vector.astype(jnp.float32)
    half_width = head_dim // 2
    turned = jnp.concatenate([rotate_half(normed[..., :half_width], grid_row, half_width), rotate_half(normed[..., half_width:], grid_col, half_width)], axis=-1)
    return turned.astype(jnp.bfloat16)

def attend(queries, key_rows, values):
    length, groups, repeats, head_dim = queries.shape
    block_rows = min(512, length)
    score_scale = head_dim ** (-0.5)

    def one_block(query_block):
        scores = jnp.einsum('qgrd,kgd->grqk', query_block.astype(jnp.float32), key_rows.astype(jnp.float32)) * score_scale
        row_max = lax.optimization_barrier(jnp.max(scores, axis=-1, keepdims=True))
        weights = jnp.exp(scores - row_max)
        row_total = lax.optimization_barrier(jnp.sum(weights, axis=-1, keepdims=True))
        rounded = weights.astype(jnp.bfloat16)
        mixed = jnp.einsum('grqk,kgd->grqd', rounded.astype(jnp.float32), values.astype(jnp.float32)) / row_total
        return jnp.transpose(mixed, (2, 0, 1, 3)).astype(jnp.bfloat16)
    blocks = queries.reshape(length // block_rows, block_rows, groups, repeats, head_dim)
    return lax.map(one_block, blocks).reshape(length, groups * repeats * head_dim)

def swiglu(row_block, gate_weight, up_weight, down_weight):
    gate_part = jnp.dot(row_block, gate_weight, preferred_element_type=jnp.float32)
    up_part = jnp.dot(row_block, up_weight, preferred_element_type=jnp.float32)
    hidden = (jax.nn.silu(gate_part) * up_part).astype(jnp.bfloat16)
    return jnp.dot(hidden, down_weight, preferred_element_type=jnp.float32)

def sequence_mixer(res_rows, query_rows, pair_rows, out_weight, norm_gain, query_gain, key_gain):
    length = query_rows.shape[0]
    kv_heads = query_rows.shape[1]
    head_dim = pair_rows.shape[2] // 2
    repeats = query_rows.shape[2] // head_dim
    position = jnp.arange(length, dtype=jnp.int32)
    grid_row = position // GRID_W
    grid_col = position % GRID_W
    queries = prepare(query_rows.reshape(length, kv_heads * repeats, head_dim), query_gain, grid_row, grid_col)
    queries = queries.reshape(length, kv_heads, repeats, head_dim)
    key_rows = prepare(pair_rows[..., :head_dim], key_gain, grid_row, grid_col)
    values = pair_rows[..., head_dim:]
    attention = attend(queries, key_rows, values)
    mixed = res_rows.astype(jnp.float32) + jnp.dot(attention, out_weight, preferred_element_type=jnp.float32)
    normed = mixed * lax.rsqrt(lax.optimization_barrier(jnp.mean(mixed * mixed, axis=-1, keepdims=True)) + norm_eps)
    normed = (normed * norm_gain.astype(jnp.float32)).astype(jnp.bfloat16)
    return (mixed, normed)

def reference(residual, query, key_value, out_weight, norm_gain, query_gain, key_gain, route_ids, route_weights, shared_gate, shared_up, shared_down, expert_gate, expert_up, expert_down):

    def one_sequence(items):
        return sequence_mixer(items[0], items[1], items[2], out_weight, norm_gain, query_gain, key_gain)
    mixed, normed = lax.map(one_sequence, (residual, query, key_value))
    model_width = residual.shape[-1]
    flat_normed = normed.reshape(-1, model_width)
    token_count = flat_normed.shape[0]
    shared = swiglu(flat_normed, shared_gate, shared_up, shared_down)
    route_list = route_ids.reshape(token_count, -1)
    raw_weights = route_weights.reshape(token_count, -1).astype(jnp.float32)
    gate_values = raw_weights / lax.optimization_barrier(jnp.sum(raw_weights, axis=-1, keepdims=True)) * routed_scale
    padded_rows = jnp.concatenate([flat_normed, jnp.zeros((1, model_width), jnp.bfloat16)], axis=0)
    most_rows = CAP * N_SP * N_DP

    def one_expert(totals, expert_id):
        hit_mask = route_list == expert_id
        weight = lax.optimization_barrier(jnp.sum(jnp.where(hit_mask, gate_values, jnp.zeros_like(gate_values)), axis=-1))
        chosen = jnp.nonzero(jnp.any(hit_mask, axis=-1), size=most_rows, fill_value=token_count)[0]
        chosen = chosen.astype(jnp.int32)
        row_block = padded_rows[chosen]
        output = swiglu(row_block, expert_gate[expert_id], expert_up[expert_id], expert_down[expert_id]).astype(jnp.bfloat16)
        weight_pad = jnp.concatenate([weight, jnp.zeros((1,), jnp.float32)], axis=0)
        totals = totals.at[chosen].add(output.astype(jnp.float32) * weight_pad[chosen][:, None])
        return (totals, None)
    routed, _ = lax.scan(one_expert, jnp.zeros((token_count + 1, model_width), jnp.float32), jnp.arange(EXPERTS, dtype=jnp.int32))
    combined = mixed.reshape(token_count, model_width) + shared + routed[:token_count]
    return combined.astype(jnp.bfloat16).reshape(residual.shape)
```

```python
import functools
import jax
import jax.numpy as jnp
from jax import lax
from jax.experimental import pallas as pl
from jax.experimental.pallas import tpu as pltpu
from jax.sharding import PartitionSpec as P

MESH = pl.DeviceIdType.MESH
N_DEV = 128
CAP = 6
SLOT = 8
GROUPS = 4
PER = N_DEV // GROUPS
GRID_W = 64
rope_theta = 10000.0
norm_eps = 1e-06
routed_scale = 2.5


def digits(n):
    return n // 32, (n // 8) % 4, (n // 2) % 4, n % 2


def shifted(me_digits, k, sign):
    d = lax.rem(k * 37, 128)
    out = []
    for m, v, size in zip(me_digits, digits(d), (4, 4, 4, 2)):
        out.append(lax.rem(m + sign * v + size, size))
    z, y, x, c = out
    return z * 4 + y, x * 2 + c


def silu_mul(g, u):
    return g / (1.0 + jnp.exp(-g)) * u


def moe_kernel(
    rows_ref, w_ref, res_ref, ngain_ref, ids_ref, rw_ref, sg_ref, su_ref, sd_ref, eg_ref, eu_ref, ed_ref,
    out_ref,
    w, sg, su, sd, eg, eu, ed, mixed, normed, g_hi, g_lo, send, recv, fout, ret, hid,
    ld_sem, s_sem, r_sem, s2_sem, r2_sem,
):
    sp = lax.axis_index("sp")
    dp = lax.axis_index("dp")
    me = (sp // 4, lax.rem(sp, 4), dp // 2, lax.rem(dp, 2))

    loads = [
        pltpu.make_async_copy(a, b, ld_sem.at[i])
        for i, (a, b) in enumerate(
            [(w_ref, w), (sg_ref, sg), (su_ref, su), (sd_ref, sd), (eg_ref.at[0], eg), (eu_ref.at[0], eu), (ed_ref.at[0], ed)]
        )
    ]
    for c in loads:
        c.start()
    barrier = pltpu.get_barrier_semaphore()

    def greet(k, c):
        pl.semaphore_signal(barrier, inc=1, device_id=shifted(me, k, 1), device_id_type=MESH)
        return c

    lax.fori_loop(1, N_DEV, greet, 0)

    lane = lax.broadcasted_iota(jnp.int32, (128, 128), 1)
    row = lax.broadcasted_iota(jnp.int32, (128, 128), 0)
    raw = rw_ref[...]
    gates = raw / jnp.sum(raw, axis=1, keepdims=True) * routed_scale
    ids = ids_ref[...]
    hit = jnp.zeros((128, 128), jnp.float32)
    gate = jnp.zeros((128, 128), jnp.float32)
    for j in range(4):
        on = ids[:, j : j + 1] == lane
        hit = hit + jnp.where(on, 1.0, 0.0)
        gate = gate + jnp.where(on, gates[:, j : j + 1], 0.0)
    hit_t = jnp.transpose(hit)
    gate_t = jnp.transpose(gate)
    before = (row < lane).astype(jnp.float32).astype(jnp.bfloat16)
    rank_t = jnp.dot(hit_t.astype(jnp.bfloat16), before, preferred_element_type=jnp.float32)
    key_t = jnp.where(hit_t > 0.0, rank_t, -1.0).astype(jnp.bfloat16)
    gate_hi = gate_t.astype(jnp.bfloat16)
    gate_lo = (gate_t - gate_hi.astype(jnp.float32)).astype(jnp.bfloat16)

    loads[0].wait()
    rows = rows_ref[...]
    total = jnp.zeros((128, 1), jnp.float32)
    for n in range(4):
        cols = pl.ds(n * 512, 512)
        part = jnp.dot(rows, w[:, cols], preferred_element_type=jnp.float32)
        part = part + res_ref[:, cols].astype(jnp.float32)
        mixed[:, cols] = part
        total = total + jnp.sum(part * part, axis=1, keepdims=True)
    scale = lax.rsqrt(total / 2048.0 + norm_eps)
    normed[...] = (mixed[...] * scale * ngain_ref[...]).astype(jnp.bfloat16)

    pl.semaphore_wait(barrier, N_DEV - 1)

    def send_copy(k):
        return pltpu.make_async_remote_copy(
            src_ref=send.at[k, pl.ds(0, CAP)], dst_ref=recv.at[k, pl.ds(0, CAP)],
            send_sem=s_sem, recv_sem=r_sem.at[k // PER],
            device_id=shifted(me, k, 1), device_id_type=MESH)

    def send_block(first, count, sem):
        at = pl.ds(first, count)
        return pltpu.make_async_remote_copy(
            src_ref=send.at[at, pl.ds(0, CAP)], dst_ref=recv.at[at, pl.ds(0, CAP)],
            send_sem=s_sem, recv_sem=sem, device_id=(sp, dp), device_id_type=MESH)

    def pack(chunk, c):
        step = chunk * 16 + row // SLOT
        d = (step * 37) & 127
        z = (me[0] + (d >> 5)) & 3
        y = (me[1] + (d >> 3)) & 3
        x = (me[2] + (d >> 1)) & 3
        co = (me[3] + d) & 1
        dest = z * 32 + y * 8 + x * 2 + co
        rep = (dest == lane).astype(jnp.float32).astype(jnp.bfloat16)
        key = jnp.dot(rep, key_t, preferred_element_type=jnp.float32)
        on = key == (row & (SLOT - 1)).astype(jnp.float32)
        pick = jnp.where(on, 1.0, 0.0).astype(jnp.bfloat16)
        hi = jnp.dot(rep, gate_hi, preferred_element_type=jnp.float32)
        lo = jnp.dot(rep, gate_lo, preferred_element_type=jnp.float32)
        at = pl.ds(pl.multiple_of(chunk * 128, 128), 128)
        g_hi[at, :] = jnp.where(on, hi, 0.0).astype(jnp.bfloat16)
        g_lo[at, :] = jnp.where(on, lo, 0.0).astype(jnp.bfloat16)
        packed = jnp.dot(pick, normed[...], preferred_element_type=jnp.float32).astype(jnp.bfloat16)
        send[pl.ds(pl.multiple_of(chunk * 16, 16), 16)] = packed.reshape(16, SLOT, 2048)

        def start(i, c):
            send_copy((chunk - 1) * 16 + i).start()
            return c

        lax.fori_loop(jnp.where(chunk == 1, 1, 0), jnp.where(chunk == 0, 0, 16), start, 0)
        return c

    lax.fori_loop(0, 8, pack, 0)
    lax.fori_loop(112, 128, lambda k, c: (send_copy(k).start(), c)[1], 0)
    recv[0] = send[0]

    for c in loads[1:4]:
        c.wait()
    xs = normed[...]
    hidden = silu_mul(
        jnp.dot(xs, sg[...], preferred_element_type=jnp.float32),
        jnp.dot(xs, su[...], preferred_element_type=jnp.float32)).astype(jnp.bfloat16)
    for n in range(4):
        cols = pl.ds(n * 512, 512)
        mixed[:, cols] = mixed[:, cols] + jnp.dot(hidden, sd[:, cols], preferred_element_type=jnp.float32)

    for c in loads[4:]:
        c.wait()

    def back_copy(k):
        return pltpu.make_async_remote_copy(
            src_ref=fout.at[k, pl.ds(0, CAP)], dst_ref=ret.at[k, pl.ds(0, CAP)],
            send_sem=s2_sem, recv_sem=r2_sem,
            device_id=shifted(me, k, -1), device_id_type=MESH)

    def expert(g, c):
        first = g * PER
        lo = jnp.where(g == 0, 1, 0)

        @pl.when(g == 0)
        def _():
            send_block(1, PER - 1, r_sem.at[0]).wait_recv()

        @pl.when(g > 0)
        def _():
            send_block(pl.multiple_of(first, PER), PER, r_sem.at[g]).wait_recv()

        at = pl.ds(pl.multiple_of(first, PER), PER)
        x = recv[at].reshape(PER * SLOT, 2048)
        hid[...] = silu_mul(
            jnp.dot(x, eg[...], preferred_element_type=jnp.float32),
            jnp.dot(x, eu[...], preferred_element_type=jnp.float32)).astype(jnp.bfloat16)
        h = hid[...]
        for n in range(4):
            cols = pl.ds(n * 512, 512)
            o = jnp.dot(h, ed[:, cols], preferred_element_type=jnp.float32).astype(jnp.bfloat16)
            fout[at, :, cols] = o.reshape(PER, SLOT, 512)

        def reply(i, c):
            back_copy(first + i).start()
            return c

        lax.fori_loop(lo, PER, reply, 0)
        return c

    lax.fori_loop(0, GROUPS, expert, 0)

    def clear(i, c):
        ret[pl.ds(pl.multiple_of(i * 16, 16), 16), pl.ds(CAP, SLOT - CAP)] = jnp.zeros((16, SLOT - CAP, 2048), jnp.bfloat16)
        return c

    lax.fori_loop(0, 8, clear, 0)
    ret[0, pl.ds(0, CAP)] = fout[0, pl.ds(0, CAP)]

    send_block(1, N_DEV - 1, r_sem.at[0]).wait_send()
    others = pl.ds(1, N_DEV - 1)
    back_all = pltpu.make_async_remote_copy(
        src_ref=fout.at[others, pl.ds(0, CAP)], dst_ref=ret.at[others, pl.ds(0, CAP)],
        send_sem=s2_sem, recv_sem=r2_sem, device_id=(sp, dp), device_id_type=MESH)
    back_all.wait_send()
    back_all.wait_recv()
    dims = (((0,), (0,)), ((), ()))
    for n in range(4):
        cols = pl.ds(n * 512, 512)
        r = ret[:, :, cols].reshape(N_DEV * SLOT, 512)
        routed = lax.dot_general(g_hi[...], r, dims, preferred_element_type=jnp.float32)
        routed = routed + lax.dot_general(g_lo[...], r, dims, preferred_element_type=jnp.float32)
        out_ref[:, cols] = (mixed[:, cols] + routed).astype(jnp.bfloat16)


def moe(rows, w, res, ngain, ids, rw, sg, su, sd, eg, eu, ed):
    bf, f32 = jnp.bfloat16, jnp.float32
    V, A = pl.BlockSpec(memory_space=pltpu.VMEM), pl.BlockSpec(memory_space=pl.ANY)
    S = pltpu.SemaphoreType.DMA
    return pl.pallas_call(
        moe_kernel,
        out_shape=jax.ShapeDtypeStruct((128, 2048), bf),
        in_specs=[V, A, V, V, V, V, A, A, A, A, A, A],
        out_specs=V,
        scratch_shapes=[
            pltpu.VMEM((2048, 2048), bf),
            pltpu.VMEM((2048, 512), bf), pltpu.VMEM((2048, 512), bf), pltpu.VMEM((512, 2048), bf),
            pltpu.VMEM((2048, 512), bf), pltpu.VMEM((2048, 512), bf), pltpu.VMEM((512, 2048), bf),
            pltpu.VMEM((128, 2048), f32), pltpu.VMEM((128, 2048), bf),
            pltpu.VMEM((1024, 128), bf), pltpu.VMEM((1024, 128), bf),
            pltpu.VMEM((128, SLOT, 2048), bf), pltpu.VMEM((128, SLOT, 2048), bf),
            pltpu.VMEM((128, SLOT, 2048), bf), pltpu.VMEM((128, SLOT, 2048), bf),
            pltpu.VMEM((PER * SLOT, 512), bf),
            S((7,)), S, S((GROUPS,)), S, S,
        ],
        compiler_params=pltpu.CompilerParams(collective_id=0, has_side_effects=True, vmem_limit_bytes=62 * 2**20),
        name="moe",
    )(rows, w, res, ngain, ids, rw, sg, su, sd, eg, eu, ed)


def rotate_half(values, position, half_width):
    inverse_freq = rope_theta ** (-jnp.arange(0, half_width, 2, dtype=jnp.float32) / half_width)
    angles = position.astype(jnp.float32)[:, None] * inverse_freq[None, :]
    angles = jnp.concatenate([angles, angles], axis=-1)
    cosine = jnp.cos(angles)[:, None, :]
    sine_part = jnp.sin(angles)[:, None, :]
    first_half, second = jnp.split(values, 2, axis=-1)
    turned = jnp.concatenate([-second, first_half], axis=-1)
    return values * cosine + turned * sine_part


def prepare(values, gain_vector, grid_row, grid_col):
    head_dim = values.shape[-1]
    floats = values.astype(jnp.float32)
    normed = floats * lax.rsqrt(jnp.mean(floats * floats, axis=-1, keepdims=True) + norm_eps)
    normed = normed * gain_vector
    half_width = head_dim // 2
    turned = jnp.concatenate(
        [
            rotate_half(normed[..., :half_width], grid_row, half_width),
            rotate_half(normed[..., half_width:], grid_col, half_width),
        ],
        axis=-1,
    )
    return turned.astype(jnp.bfloat16)


def attend(queries, key_rows, values):
    length, groups, repeats, head_dim = queries.shape
    block_rows = min(512, length)
    score_scale = head_dim ** (-0.5)

    def one_block(query_block):
        scores = (
            jnp.einsum("qgrd,kgd->grqk", query_block, key_rows, preferred_element_type=jnp.float32)
            * score_scale
        )
        row_max = jnp.max(scores, axis=-1, keepdims=True)
        weights = jnp.exp(scores - row_max)
        row_total = jnp.sum(weights, axis=-1, keepdims=True)
        rounded = weights.astype(jnp.bfloat16)
        mixed = (
            jnp.einsum("grqk,kgd->grqd", rounded, values, preferred_element_type=jnp.float32)
            / row_total
        )
        return jnp.transpose(mixed, (2, 0, 1, 3)).astype(jnp.bfloat16)

    blocks = queries.reshape(length // block_rows, block_rows, groups, repeats, head_dim)
    return lax.map(one_block, blocks).reshape(length, groups * repeats * head_dim)


def swiglu(row_block, gate_weight, up_weight, down_weight):
    gate_part = jnp.dot(row_block, gate_weight, preferred_element_type=jnp.float32)
    up_part = jnp.dot(row_block, up_weight, preferred_element_type=jnp.float32)
    hidden = (jax.nn.silu(gate_part) * up_part).astype(jnp.bfloat16)
    return jnp.dot(hidden, down_weight, preferred_element_type=jnp.float32)


def per_device(
    residual,
    query,
    key_value,
    out_weight,
    norm_gain,
    query_gain,
    key_gain,
    route_ids,
    route_weights,
    shared_gate,
    shared_up,
    shared_down,
    expert_gate,
    expert_up,
    expert_down,
):
    tokens = residual.shape[1]
    model_width = residual.shape[2]
    head_dim = key_value.shape[3] // 2
    head_rows, pair_rows = (
        lax.all_to_all(query, "sp", split_axis=2, concat_axis=1, tiled=True),
        lax.all_to_all(key_value, "sp", split_axis=2, concat_axis=1, tiled=True),
    )
    length = head_rows.shape[1]
    kv_local = head_rows.shape[2]
    repeats = head_rows.shape[3] // head_dim
    position = jnp.arange(length, dtype=jnp.int32)
    grid_row = position // GRID_W
    grid_col = position % GRID_W
    queries = prepare(
        head_rows[0].reshape(length, kv_local * repeats, head_dim), query_gain, grid_row, grid_col
    )
    queries = queries.reshape(length, kv_local, repeats, head_dim)
    key_rows = prepare(pair_rows[0][..., :head_dim], key_gain, grid_row, grid_col)
    values = pair_rows[0][..., head_dim:]
    attention = attend(queries, key_rows, values)
    returned_heads = lax.all_to_all(
        attention.reshape(1, length, kv_local, repeats * head_dim),
        "sp",
        split_axis=1,
        concat_axis=2,
        tiled=True,
    )
    flat_rows = returned_heads.reshape(tokens, -1)
    full_weight = lax.all_gather(out_weight, "dp", axis=1, tiled=True)
    combined = moe(
        flat_rows, full_weight, residual[0], norm_gain[None, :], route_ids[0], route_weights[0],
        shared_gate, shared_up, shared_down, expert_gate, expert_up, expert_down,
    )
    return combined.reshape(1, tokens, model_width)


def solution(mesh):
    in_specs = (
        P("dp", "sp", None),
        P("dp", "sp", None, None),
        P("dp", "sp", None, None),
        P(None, "dp"),
        P(),
        P(),
        P(),
        P("dp", "sp", None),
        P("dp", "sp", None),
        P(),
        P(),
        P(),
        P(("sp", "dp"), None, None),
        P(("sp", "dp"), None, None),
        P(("sp", "dp"), None, None),
    )
    out_specs = P("dp", "sp", None)
    return jax.shard_map(
        per_device, mesh=mesh, in_specs=in_specs, out_specs=out_specs, check_vma=False
    )
```

```python
import math
import jax
import jax.numpy as jnp
from jax import lax
from jax.experimental import pallas as pl
from jax.experimental.pallas import tpu as pltpu
import numpy as np
from jax.sharding import PartitionSpec as P

MESH = pl.DeviceIdType.MESH
N_DEV = 128
CAP = 6
SLOT = 8
GROUPS = 4
PER = N_DEV // GROUPS
norm_eps = 1e-06
rope_theta = 10000.0
routed_scale = 2.5
N_SP = 16
LEN = 2048
BLOCKS = 8
EXP_SCALE = 0.125 * math.log2(math.e)


def digits(n):
    return n // 32, (n // 8) % 4, (n // 2) % 4, n % 2


def shifted(me_digits, k, sign):
    d = lax.rem(k * 37, 128)
    out = []
    for m, v, size in zip(me_digits, digits(d), (4, 4, 4, 2)):
        out.append(lax.rem(m + sign * v + size, size))
    z, y, x, c = out
    return z * 4 + y, x * 2 + c


def silu_mul(g, u):
    return g / (1.0 + jnp.exp(-g)) * u


def sp_shifted(me, k, sign):
    d = lax.rem(k * 7, 16)
    z = lax.rem(me[0] + sign * (d // 4) + 4, 4)
    y = lax.rem(me[1] + sign * lax.rem(d, 4) + 4, 4)
    return z * 4 + y


def rope_tables():
    lanes = np.arange(128)
    theta = (np.float32(rope_theta) ** (-(2 * (lanes % 16)).astype(np.float32) / np.float32(32))).astype(np.float32)
    angles = np.arange(64, dtype=np.float32)[:, None] * theta[None, :]
    sign = np.where(lanes % 32 < 16, -1.0, 1.0)
    return np.cos(angles).astype(np.float32), (np.sin(angles) * sign).astype(np.float32)


def layer_kernel(
    q_ref, kv_ref, cos_ref, sin_ref, qg_ref, kg_ref,
    w_ref, res_ref, ngain_ref, ids_ref, rw_ref, sg_ref, su_ref, sd_ref, eg_ref, eu_ref, ed_ref,
    out_ref,
    w, sg, su, sd, eg, eu, ed, mixed, normed, g_hi, g_lo, send, recv, fout, ret, hid,
    wide, sq, skv, rq, rkv, kt, vx, ao, rows,
    ld_sem, s_sem, r_sem, s2_sem, r2_sem, kvs_sem, kvr_sem, qs_sem, qr_sem, bs_sem, br_sem, ws_sem, wr_sem,
):
    sp = lax.axis_index("sp")
    dp = lax.axis_index("dp")
    me = (sp // 4, lax.rem(sp, 4), dp // 2, lax.rem(dp, 2))

    own_cols = pl.ds(pl.multiple_of(dp * 256, 256), 256)
    loads = [
        pltpu.make_async_copy(a, b, ld_sem.at[i])
        for i, (a, b) in enumerate(
            [(w_ref, w.at[:, own_cols]), (sg_ref, sg), (su_ref, su), (sd_ref, sd), (eg_ref.at[0], eg), (eu_ref.at[0], eu), (ed_ref.at[0], ed)]
        )
    ]
    for c in loads:
        c.start()
    barrier = pltpu.get_barrier_semaphore()

    def greet(k, c):
        pl.semaphore_signal(barrier, inc=1, device_id=shifted(me, k, 1), device_id_type=MESH)
        return c

    lax.fori_loop(1, N_DEV, greet, 0)

    lane = lax.broadcasted_iota(jnp.int32, (128, 128), 1)
    row = lax.broadcasted_iota(jnp.int32, (128, 128), 0)

    lane1 = lax.broadcasted_iota(jnp.int32, (1, 128), 1)
    swap_up = (lane1 & 31) < 16

    def turned_gain(g):
        return jnp.where(swap_up, pltpu.roll(g, 112, 1), pltpu.roll(g, 16, 1))

    def both(g):
        return jnp.concatenate([g, g], axis=1)

    col_lane = (lane1 & 63) >= 32
    first = pl.ds(0, 64)
    second = pl.ds(64, 64)
    q_gain, k_gain = both(qg_ref[...]), both(kg_ref[...])
    q_gain8, k_gain8 = jnp.broadcast_to(q_gain, (8, 128)), jnp.broadcast_to(k_gain, (8, 128))
    q_turn, k_turn = turned_gain(q_gain8)[0:1], turned_gain(k_gain8)[0:1]

    def table(ref):
        top = jnp.where(col_lane, ref[...], ref[pl.ds(sp * 2, 1), :])
        bottom = jnp.where(col_lane, ref[...], ref[pl.ds(sp * 2 + 1, 1), :])
        return jnp.concatenate([top, bottom], axis=0)

    cosine, sine = table(cos_ref), table(sin_ref)
    ones_block = ((row >> 6) == (lane >> 6)).astype(jnp.float32).astype(jnp.bfloat16)
    turn = ((row ^ 16) == lane).astype(jnp.float32).astype(jnp.bfloat16)

    def prepared(x, cos_gain, sin_gain):
        xb = x.astype(jnp.bfloat16)
        square = x * x
        high = square.astype(jnp.bfloat16)
        low = (square - high.astype(jnp.float32)).astype(jnp.bfloat16)
        total = jnp.dot(high, ones_block, preferred_element_type=jnp.float32)
        total = total + jnp.dot(low, ones_block, preferred_element_type=jnp.float32)
        other = jnp.dot(xb, turn, preferred_element_type=jnp.float32)
        return lax.rsqrt(total / 64.0 + norm_eps) * (x * cos_gain + other * sin_gain)

    def prepare_all(source, target, cos_gain, sin_gain, keep):
        wide[...] = source[...].astype(jnp.float32).reshape(LEN, 128)

        def one(k, c):
            x = wide[pl.ds(sp_shifted(me, k, 1), 128, stride=16), :]
            y = prepared(x, cos_gain, sin_gain)
            if keep:
                y = jnp.where(lane < 64, y, x)
            target[k] = y.astype(jnp.bfloat16)
            return c

        lax.fori_loop(0, N_SP, one, 0)

    prepare_all(kv_ref, skv, cosine * k_gain, sine * k_turn, True)
    prepare_all(q_ref, sq, cosine * q_gain, sine * q_turn, False)

    pl.semaphore_wait(barrier, N_DEV - 1)

    def sp_copy(src, dst, k, sign, s, r):
        return pltpu.make_async_remote_copy(
            src_ref=src, dst_ref=dst, send_sem=s, recv_sem=r,
            device_id=(sp_shifted(me, k, sign), dp), device_id_type=MESH)

    def send_kv(k, c):
        sp_copy(skv.at[k], rkv.at[k], k, 1, kvs_sem, kvr_sem).start()
        return c

    def send_q(k, c):
        sp_copy(sq.at[k], rq.at[k], k, 1, qs_sem, qr_sem.at[k // 2]).start()
        return c

    lax.fori_loop(1, N_SP, send_kv, 0)
    lax.fori_loop(1, N_SP, send_q, 0)

    loads[0].wait()
    x_at, core = me[2], me[3]
    right, left = lax.rem(x_at + 1, 4), lax.rem(x_at + 3, 4)

    def w_copy(x_from, core_from, half, x_to, core_to, number):
        size = LEN if half is None else LEN // 2
        at = w.at[pl.ds(0 if half is None else half * size, size), pl.ds(pl.multiple_of((x_from * 2 + core_from) * 256, 256), 256)]
        return pltpu.make_async_remote_copy(
            src_ref=at, dst_ref=at, send_sem=ws_sem, recv_sem=wr_sem.at[number],
            device_id=(sp, x_to * 2 + core_to), device_id_type=MESH)

    w_copy(x_at, core, 0, right, core, 0).start()
    w_copy(x_at, core, 1, left, core, 1).start()
    w_copy(x_at, core, 1, right, core, 2).start()
    w_copy(x_at, core, 0, left, core, 3).start()
    w_copy(x_at, core, None, x_at, 1 - core, 4).start()
    far = lax.rem(x_at + 2, 4)
    early = ((left, 0, 0), (right, 1, 1))
    later = ((left, 1, 2), (right, 0, 3))
    last = ((far, 0, 5), (far, 1, 6))

    def w_relay():
        for x_from, half, number in early:
            w_copy(x_from, core, half, right, core, number).wait_recv()
        w_copy(left, core, 0, right, core, 5).start()
        w_copy(right, core, 1, left, core, 6).start()
        for x_from, half, number in early:
            w_copy(x_from, core, half, x_at, 1 - core, 7 + number).start()

    def w_share(some):
        for x_from, half, number in some:
            w_copy(x_from, core, half, right, core, number).wait_recv()
            w_copy(x_from, core, half, x_at, 1 - core, 7 + number).start()

    def w_finish():
        w_copy(x_at, 1 - core, None, x_at, core, 4).wait_recv()
        for x_from, half, number in early + later + last:
            w_copy(x_from, 1 - core, half, x_at, core, 7 + number).wait_recv()
        everything = w.at[:, pl.ds(0, 7 * 256)]
        pltpu.make_async_remote_copy(
            src_ref=everything, dst_ref=everything, send_sem=ws_sem, recv_sem=wr_sem.at[0],
            device_id=(sp, dp), device_id_type=MESH).wait_send()

    raw = rw_ref[...]
    gates = raw / jnp.sum(raw, axis=1, keepdims=True) * routed_scale
    ids = ids_ref[...]
    hit = jnp.zeros((128, 128), jnp.float32)
    gate = jnp.zeros((128, 128), jnp.float32)
    for j in range(4):
        on = ids[:, j : j + 1] == lane
        hit = hit + jnp.where(on, 1.0, 0.0)
        gate = gate + jnp.where(on, gates[:, j : j + 1], 0.0)
    hit_t = jnp.transpose(hit)
    gate_t = jnp.transpose(gate)
    before = (row < lane).astype(jnp.float32).astype(jnp.bfloat16)
    rank_t = jnp.dot(hit_t.astype(jnp.bfloat16), before, preferred_element_type=jnp.float32)
    key_t = jnp.where(hit_t > 0.0, rank_t, -1.0).astype(jnp.bfloat16)
    gate_hi = gate_t.astype(jnp.bfloat16)
    gate_lo = (gate_t - gate_hi.astype(jnp.float32)).astype(jnp.bfloat16)

    def clear(i, c):
        ret[pl.ds(pl.multiple_of(i * 16, 16), 16), pl.ds(CAP, SLOT - CAP)] = jnp.zeros((16, SLOT - CAP, 2048), jnp.bfloat16)
        return c

    lax.fori_loop(0, 8, clear, 0)

    rkv[0] = skv[0]
    rq[0] = sq[0]
    others16 = pl.ds(1, N_SP - 1)

    def sp_all(src, dst, s, r):
        return pltpu.make_async_remote_copy(
            src_ref=src, dst_ref=dst, send_sem=s, recv_sem=r, device_id=(sp, dp), device_id_type=MESH)

    sp_all(skv.at[others16], rkv.at[others16], kvs_sem, kvr_sem).wait_recv()

    def lay(k, c):
        pair = rkv[k].astype(jnp.float32)
        swapped = pltpu.roll(pair, 64, 1)
        low_lane = lane < 64
        at = pl.ds(pl.multiple_of(k * 128, 128), 128)
        at2 = pl.ds(pl.multiple_of(LEN + k * 128, 128), 128)
        kt[:, at] = jnp.transpose(jnp.where(low_lane, pair, 0.0)).astype(jnp.bfloat16)
        kt[:, at2] = jnp.transpose(jnp.where(low_lane, 0.0, swapped)).astype(jnp.bfloat16)
        vx[at, pl.ds(0, 128)] = jnp.where(low_lane, swapped, 0.0).astype(jnp.bfloat16)
        vx[at2, pl.ds(0, 128)] = jnp.where(low_lane, 0.0, pair).astype(jnp.bfloat16)
        vx[at, pl.ds(128, 128)] = jnp.where(low_lane, 1.0, 0.0).astype(jnp.bfloat16)
        vx[at2, pl.ds(128, 128)] = jnp.where(low_lane, 0.0, 1.0).astype(jnp.bfloat16)
        return c

    lax.fori_loop(0, N_SP, lay, 0)
    own_rows = pl.ds(pl.multiple_of(sp * 128, 128), 128)

    def back_rows(k):
        return sp_copy(ao.at[k], rows.at[:, own_rows], k, -1, bs_sem, br_sem)

    def block(b, c):
        @pl.when(b == 0)
        def _():
            sp_all(sq.at[1], rq.at[1], qs_sem, qr_sem.at[0]).wait_recv()

        @pl.when(b > 0)
        def _():
            two = pl.ds(b * 2, 2)
            sp_all(sq.at[two], rq.at[two], qs_sem, qr_sem.at[b]).wait_recv()

        q = rq[pl.ds(b * 2, 2)].reshape(256, 128)
        o = jnp.zeros((256, 256), jnp.float32)
        for h in range(2):
            keys = pl.ds(h * LEN, LEN)
            s = jnp.dot(q, kt[:, keys], preferred_element_type=jnp.float32)
            top = jnp.max(s, axis=1, keepdims=True)
            p = jnp.exp2((s - top) * EXP_SCALE).astype(jnp.bfloat16)
            o = o + jnp.dot(p, vx[keys, :], preferred_element_type=jnp.float32)
        a = (o[:, :128] / o[:, 128:]).astype(jnp.bfloat16)
        ao[pl.ds(b * 2, 2)] = a.reshape(2, 128, 128)

        @pl.when(b > 0)
        def _():
            back_rows(b * 2).start()

        back_rows(b * 2 + 1).start()

        @pl.when(b == 4)
        def _():
            w_relay()

        return c

    lax.fori_loop(0, BLOCKS, block, 0)
    rows[:, own_rows] = ao[0]
    sp_all(skv.at[others16], rkv.at[others16], kvs_sem, kvr_sem).wait_send()
    sp_all(sq.at[others16], rq.at[others16], qs_sem, qr_sem.at[0]).wait_send()
    w_share(later)
    w_share(last)
    w_finish()
    back_all16 = sp_all(ao.at[others16], ao.at[others16], bs_sem, br_sem)
    back_all16.wait_send()
    back_all16.wait_recv()

    total = jnp.zeros((128, 1), jnp.float32)
    for n in range(4):
        cols = pl.ds(n * 512, 512)
        part = jnp.dot(rows[...], w[:, cols], preferred_element_type=jnp.float32)
        part = part + res_ref[:, cols].astype(jnp.float32)
        mixed[:, cols] = part
        total = total + jnp.sum(part * part, axis=1, keepdims=True)
    scale = lax.rsqrt(total / 2048.0 + norm_eps)
    normed[...] = (mixed[...] * scale * ngain_ref[...]).astype(jnp.bfloat16)

    def send_copy(k):
        return pltpu.make_async_remote_copy(
            src_ref=send.at[k, pl.ds(0, CAP)], dst_ref=recv.at[k, pl.ds(0, CAP)],
            send_sem=s_sem, recv_sem=r_sem.at[k // PER],
            device_id=shifted(me, k, 1), device_id_type=MESH)

    def send_block(first, count, sem):
        at = pl.ds(first, count)
        return pltpu.make_async_remote_copy(
            src_ref=send.at[at, pl.ds(0, CAP)], dst_ref=recv.at[at, pl.ds(0, CAP)],
            send_sem=s_sem, recv_sem=sem, device_id=(sp, dp), device_id_type=MESH)

    def pack(chunk, c):
        step = chunk * 16 + row // SLOT
        d = (step * 37) & 127
        z = (me[0] + (d >> 5)) & 3
        y = (me[1] + (d >> 3)) & 3
        x = (me[2] + (d >> 1)) & 3
        co = (me[3] + d) & 1
        dest = z * 32 + y * 8 + x * 2 + co
        rep = (dest == lane).astype(jnp.float32).astype(jnp.bfloat16)
        key = jnp.dot(rep, key_t, preferred_element_type=jnp.float32)
        on = key == (row & (SLOT - 1)).astype(jnp.float32)
        pick = jnp.where(on, 1.0, 0.0).astype(jnp.bfloat16)
        hi = jnp.dot(rep, gate_hi, preferred_element_type=jnp.float32)
        lo = jnp.dot(rep, gate_lo, preferred_element_type=jnp.float32)
        at = pl.ds(pl.multiple_of(chunk * 128, 128), 128)
        g_hi[at, :] = jnp.where(on, hi, 0.0).astype(jnp.bfloat16)
        g_lo[at, :] = jnp.where(on, lo, 0.0).astype(jnp.bfloat16)
        packed = jnp.dot(pick, normed[...], preferred_element_type=jnp.float32).astype(jnp.bfloat16)
        send[pl.ds(pl.multiple_of(chunk * 16, 16), 16)] = packed.reshape(16, SLOT, 2048)

        def start(i, c):
            send_copy((chunk - 1) * 16 + i).start()
            return c

        lax.fori_loop(jnp.where(chunk == 1, 1, 0), jnp.where(chunk == 0, 0, 16), start, 0)
        return c

    lax.fori_loop(0, 8, pack, 0)
    lax.fori_loop(112, 128, lambda k, c: (send_copy(k).start(), c)[1], 0)
    recv[0] = send[0]

    for c in loads[1:4]:
        c.wait()
    xs = normed[...]
    hidden = silu_mul(
        jnp.dot(xs, sg[...], preferred_element_type=jnp.float32),
        jnp.dot(xs, su[...], preferred_element_type=jnp.float32)).astype(jnp.bfloat16)
    for n in range(4):
        cols = pl.ds(n * 512, 512)
        mixed[:, cols] = mixed[:, cols] + jnp.dot(hidden, sd[:, cols], preferred_element_type=jnp.float32)

    for c in loads[4:]:
        c.wait()

    def back_copy(k):
        return pltpu.make_async_remote_copy(
            src_ref=fout.at[k, pl.ds(0, CAP)], dst_ref=ret.at[k, pl.ds(0, CAP)],
            send_sem=s2_sem, recv_sem=r2_sem,
            device_id=shifted(me, k, -1), device_id_type=MESH)

    def expert(g, c):
        first = g * PER
        lo = jnp.where(g == 0, 1, 0)

        @pl.when(g == 0)
        def _():
            send_block(1, PER - 1, r_sem.at[0]).wait_recv()

        @pl.when(g > 0)
        def _():
            send_block(pl.multiple_of(first, PER), PER, r_sem.at[g]).wait_recv()

        at = pl.ds(pl.multiple_of(first, PER), PER)
        x = recv[at].reshape(PER * SLOT, 2048)
        hid[...] = silu_mul(
            jnp.dot(x, eg[...], preferred_element_type=jnp.float32),
            jnp.dot(x, eu[...], preferred_element_type=jnp.float32)).astype(jnp.bfloat16)
        h = hid[...]
        for n in range(4):
            cols = pl.ds(n * 512, 512)
            o = jnp.dot(h, ed[:, cols], preferred_element_type=jnp.float32).astype(jnp.bfloat16)
            fout[at, :, cols] = o.reshape(PER, SLOT, 512)

        def reply(i, c):
            back_copy(first + i).start()
            return c

        lax.fori_loop(lo, PER, reply, 0)
        return c

    lax.fori_loop(0, GROUPS, expert, 0)

    ret[0, pl.ds(0, CAP)] = fout[0, pl.ds(0, CAP)]

    send_block(1, N_DEV - 1, r_sem.at[0]).wait_send()
    others = pl.ds(1, N_DEV - 1)
    back_all = pltpu.make_async_remote_copy(
        src_ref=fout.at[others, pl.ds(0, CAP)], dst_ref=ret.at[others, pl.ds(0, CAP)],
        send_sem=s2_sem, recv_sem=r2_sem, device_id=(sp, dp), device_id_type=MESH)
    back_all.wait_send()
    back_all.wait_recv()
    dims = (((0,), (0,)), ((), ()))
    for n in range(4):
        cols = pl.ds(n * 512, 512)
        r = ret[:, :, cols].reshape(N_DEV * SLOT, 512)
        routed = lax.dot_general(g_hi[...], r, dims, preferred_element_type=jnp.float32)
        routed = routed + lax.dot_general(g_lo[...], r, dims, preferred_element_type=jnp.float32)
        out_ref[:, cols] = (mixed[:, cols] + routed).astype(jnp.bfloat16)


def layer(*operands):
    bf, f32 = jnp.bfloat16, jnp.float32
    V, A = pl.BlockSpec(memory_space=pltpu.VMEM), pl.BlockSpec(memory_space=pl.ANY)
    S = pltpu.SemaphoreType.DMA
    M = pltpu.VMEM
    return pl.pallas_call(
        layer_kernel,
        out_shape=jax.ShapeDtypeStruct((128, 2048), bf),
        in_specs=[V, V, V, V, V, V, A, V, V, V, V, A, A, A, A, A, A],
        out_specs=V,
        scratch_shapes=[
            M((2048, 2048), bf),
            M((2048, 512), bf), M((2048, 512), bf), M((512, 2048), bf),
            M((2048, 512), bf), M((2048, 512), bf), M((512, 2048), bf),
            M((128, 2048), f32), M((128, 2048), bf),
            M((1024, 128), bf), M((1024, 128), bf),
            M((128, SLOT, 2048), bf), M((128, SLOT, 2048), bf),
            M((128, SLOT, 2048), bf), M((128, SLOT, 2048), bf),
            M((PER * SLOT, 512), bf),
            M((LEN, 128), f32), M((N_SP, 128, 128), bf), M((N_SP, 128, 128), bf), M((N_SP, 128, 128), bf),
            M((N_SP, 128, 128), bf), M((128, 2 * LEN), bf), M((2 * LEN, 256), bf), M((N_SP, 128, 128), bf),
            M((128, 2048), bf),
            S((7,)), S, S((GROUPS,)), S, S, S, S, S, S((BLOCKS,)), S, S, S, S((14,)),
        ],
        compiler_params=pltpu.CompilerParams(collective_id=0, has_side_effects=True, vmem_limit_bytes=63 * 2**20),
        name="layer",
    )(*operands)


def per_device(
    residual, query, key_value, out_weight, norm_gain, query_gain, key_gain, route_ids, route_weights,
    shared_gate, shared_up, shared_down, expert_gate, expert_up, expert_down,
):
    cosine, sine = rope_tables()
    combined = layer(
        query[0], key_value[0], jnp.asarray(cosine), jnp.asarray(sine), query_gain[None, :], key_gain[None, :],
        out_weight, residual[0], norm_gain[None, :], route_ids[0], route_weights[0],
        shared_gate, shared_up, shared_down, expert_gate, expert_up, expert_down,
    )
    return combined[None]


def solution(mesh):
    in_specs = (
        P("dp", "sp", None),
        P("dp", "sp", None, None),
        P("dp", "sp", None, None),
        P(None, "dp"),
        P(),
        P(),
        P(),
        P("dp", "sp", None),
        P("dp", "sp", None),
        P(),
        P(),
        P(),
        P(("sp", "dp"), None, None),
        P(("sp", "dp"), None, None),
        P(("sp", "dp"), None, None),
    )
    out_specs = P("dp", "sp", None)
    return jax.shard_map(
        per_device, mesh=mesh, in_specs=in_specs, out_specs=out_specs, check_vma=False
    )
```

```python
import math
import jax
import jax.numpy as jnp
from jax import lax
from jax.experimental import pallas as pl
from jax.experimental.pallas import tpu as pltpu
import numpy as np
from jax.sharding import PartitionSpec as P

MESH = pl.DeviceIdType.MESH
N_DEV = 128
CAP = 6
SLOT = 8
GROUPS = 4
PER = N_DEV // GROUPS
norm_eps = 1e-06
rope_theta = 10000.0
routed_scale = 2.5
N_SP = 16
LEN = 2048
BLOCKS = 8
HEADS = 4
STRIDE = 91
KEYS = 512
EXP_SCALE = 0.125 * math.log2(math.e)


def digits(n):
    return n // 32, (n // 8) % 4, (n // 2) % 4, n % 2


def shifted(me_digits, k, sign):
    d = lax.rem(k * STRIDE, 128)
    out = []
    for m, v, size in zip(me_digits, digits(d), (4, 4, 4, 2)):
        out.append(lax.rem(m + sign * v + size, size))
    z, y, x, c = out
    return z * 4 + y, x * 2 + c


def silu_mul(g, u):
    return g / (1.0 + jnp.exp(-g)) * u


def sp_shifted(me, k, sign):
    d = lax.rem(k * 7, 16)
    z = lax.rem(me[0] + sign * (d // 4) + 4, 4)
    y = lax.rem(me[1] + sign * lax.rem(d, 4) + 4, 4)
    return z * 4 + y


def rope_tables():
    lanes = np.arange(128)
    theta = (np.float32(rope_theta) ** (-(2 * (lanes % 16)).astype(np.float32) / np.float32(32))).astype(np.float32)
    angles = np.arange(64, dtype=np.float32)[:, None] * theta[None, :]
    sign = np.where(lanes % 32 < 16, -1.0, 1.0)
    return np.cos(angles).astype(np.float32), (np.sin(angles) * sign).astype(np.float32)


def layer_kernel(
    q_ref, kv_ref, cos_ref, sin_ref, qg_ref, kg_ref,
    w_ref, res_ref, ngain_ref, ids_ref, rw_ref, sg_ref, su_ref, sd_ref, eg_ref, eu_ref, ed_ref,
    out_ref,
    w, sg, su, sd, eg, eu, ed, mixed, normed, g_hi, g_lo, pick, send, recv, fout, ret, hid,
    wide, sq, skv, rq, rkv, kt, vx, ao, rows, s_even, s_odd, peak_even, peak_odd,
    ld_sem, s_sem, r_sem, s2_sem, r2_sem, kvs_sem, kvr_sem, qs_sem, qr_sem, bs_sem, br_sem, ws_sem, wr_sem,
):
    sp = lax.axis_index("sp")
    dp = lax.axis_index("dp")
    me = (sp // 4, lax.rem(sp, 4), dp // 2, lax.rem(dp, 2))

    own_cols = pl.ds(pl.multiple_of(dp * 256, 256), 256)
    loads = [
        pltpu.make_async_copy(a, b, ld_sem.at[i])
        for i, (a, b) in enumerate(
            [(w_ref, w.at[:, own_cols]), (sg_ref, sg), (su_ref, su), (sd_ref, sd), (eg_ref.at[0], eg), (eu_ref.at[0], eu), (ed_ref.at[0], ed)]
        )
    ]
    for c in loads:
        c.start()
    barrier = pltpu.get_barrier_semaphore()

    sp_of = [((me[0] + i // 4) & 3) * 4 + ((me[1] + i % 4) & 3) for i in range(N_SP)]
    dp_of = [((me[2] + i // 2) & 3) * 2 + ((me[3] + i % 2) & 1) for i in range(8)]
    for i in range(1, N_DEV):
        pl.semaphore_signal(barrier, inc=1, device_id=(sp_of[i // 8], dp_of[i % 8]), device_id_type=MESH)

    lane = lax.broadcasted_iota(jnp.int32, (128, 128), 1)
    row = lax.broadcasted_iota(jnp.int32, (128, 128), 0)

    lane1 = lax.broadcasted_iota(jnp.int32, (1, 128), 1)
    swap_up = (lane1 & 31) < 16

    def turned_gain(g):
        return jnp.where(swap_up, pltpu.roll(g, 112, 1), pltpu.roll(g, 16, 1))

    def both(g):
        return jnp.concatenate([g, g], axis=1)

    col_lane = (lane1 & 63) >= 32
    first = pl.ds(0, 64)
    second = pl.ds(64, 64)
    q_gain, k_gain = both(qg_ref[...]), both(kg_ref[...])
    q_gain8, k_gain8 = jnp.broadcast_to(q_gain, (8, 128)), jnp.broadcast_to(k_gain, (8, 128))
    q_turn, k_turn = turned_gain(q_gain8)[0:1], turned_gain(k_gain8)[0:1]

    def table(ref):
        top = jnp.where(col_lane, ref[...], ref[pl.ds(sp * 2, 1), :])
        bottom = jnp.where(col_lane, ref[...], ref[pl.ds(sp * 2 + 1, 1), :])
        return jnp.concatenate([top, bottom], axis=0)

    cosine, sine = table(cos_ref), table(sin_ref)
    ones_block = ((row >> 6) == (lane >> 6)).astype(jnp.float32).astype(jnp.bfloat16)
    turn = ((row ^ 16) == lane).astype(jnp.float32).astype(jnp.bfloat16)

    def prepared(x, cos_gain, sin_gain):
        xb = x.astype(jnp.bfloat16)
        square = x * x
        high = square.astype(jnp.bfloat16)
        low = (square - high.astype(jnp.float32)).astype(jnp.bfloat16)
        total = jnp.dot(high, ones_block, preferred_element_type=jnp.float32)
        total = total + jnp.dot(low, ones_block, preferred_element_type=jnp.float32)
        other = jnp.dot(xb, turn, preferred_element_type=jnp.float32)
        return lax.rsqrt(total / 64.0 + norm_eps) * (x * cos_gain + other * sin_gain)

    def prepare_all(source, target, cos_gain, sin_gain, keep):
        wide[...] = source[...].astype(jnp.float32).reshape(LEN, 128)

        def some(g, c):
            x = jnp.concatenate(
                [wide[pl.ds(sp_shifted(me, g * HEADS + i, 1), 128, stride=16), :] for i in range(HEADS)], axis=0)
            y = prepared(x, cos_gain, sin_gain)
            if keep:
                y = jnp.where(jnp.broadcast_to(lane1 < 64, y.shape), y, x)
            target[pl.ds(g * HEADS, HEADS)] = y.astype(jnp.bfloat16).reshape(HEADS, 128, 128)
            return c

        lax.fori_loop(0, N_SP // HEADS, some, 0)

    def stacked(t):
        return jnp.concatenate([t] * HEADS, axis=0)

    prepare_all(kv_ref, skv, stacked(cosine * k_gain), stacked(sine * k_turn), True)
    prepare_all(q_ref, sq, stacked(cosine * q_gain), stacked(sine * q_turn), False)

    pl.semaphore_wait(barrier, N_DEV - 1)

    def sp_copy(src, dst, k, sign, s, r):
        return pltpu.make_async_remote_copy(
            src_ref=src, dst_ref=dst, send_sem=s, recv_sem=r,
            device_id=(sp_shifted(me, k, sign), dp), device_id_type=MESH)

    def send_kv(k, c):
        sp_copy(skv.at[k], rkv.at[k], k, 1, kvs_sem, kvr_sem).start()
        return c

    def send_q(k, c):
        sp_copy(sq.at[k], rq.at[k], k, 1, qs_sem, qr_sem.at[k // 2]).start()
        return c

    lax.fori_loop(1, N_SP, send_kv, 0)

    loads[0].wait()
    x_at, core = me[2], me[3]
    right, left = lax.rem(x_at + 1, 4), lax.rem(x_at + 3, 4)

    def w_copy(x_from, core_from, half, x_to, core_to, number):
        size = LEN if half is None else LEN // 2
        at = w.at[pl.ds(0 if half is None else half * size, size), pl.ds(pl.multiple_of((x_from * 2 + core_from) * 256, 256), 256)]
        return pltpu.make_async_remote_copy(
            src_ref=at, dst_ref=at, send_sem=ws_sem, recv_sem=wr_sem.at[number],
            device_id=(sp, x_to * 2 + core_to), device_id_type=MESH)

    w_copy(x_at, core, 0, right, core, 0).start()
    w_copy(x_at, core, 1, left, core, 1).start()
    w_copy(x_at, core, 1, right, core, 2).start()
    w_copy(x_at, core, 0, left, core, 3).start()
    w_copy(x_at, core, None, x_at, 1 - core, 4).start()
    far = lax.rem(x_at + 2, 4)
    early = ((left, 0, 0), (right, 1, 1))
    later = ((left, 1, 2), (right, 0, 3))
    last = ((far, 0, 5), (far, 1, 6))

    def w_relay():
        for x_from, half, number in early:
            w_copy(x_from, core, half, right, core, number).wait_recv()
        w_copy(left, core, 0, right, core, 5).start()
        w_copy(right, core, 1, left, core, 6).start()
        for x_from, half, number in early:
            w_copy(x_from, core, half, x_at, 1 - core, 7 + number).start()

    def w_share(some):
        for x_from, half, number in some:
            w_copy(x_from, core, half, right, core, number).wait_recv()
            w_copy(x_from, core, half, x_at, 1 - core, 7 + number).start()

    def w_finish():
        w_copy(x_at, 1 - core, None, x_at, core, 4).wait_recv()
        for x_from, half, number in early + later + last:
            w_copy(x_from, 1 - core, half, x_at, core, 7 + number).wait_recv()
        everything = w.at[:, pl.ds(0, 7 * 256)]
        pltpu.make_async_remote_copy(
            src_ref=everything, dst_ref=everything, send_sem=ws_sem, recv_sem=wr_sem.at[0],
            device_id=(sp, dp), device_id_type=MESH).wait_send()

    raw = rw_ref[...]
    gates = raw / jnp.sum(raw, axis=0, keepdims=True) * routed_scale
    ids = ids_ref[...]
    hit_t = jnp.zeros((128, 128), jnp.float32)
    gate_t = jnp.zeros((128, 128), jnp.float32)
    for j in range(4):
        on = ids[j : j + 1, :] == row
        hit_t = hit_t + jnp.where(on, 1.0, 0.0)
        gate_t = gate_t + jnp.where(on, gates[j : j + 1, :], 0.0)
    before = (row < lane).astype(jnp.float32).astype(jnp.bfloat16)
    rank_t = jnp.dot(hit_t.astype(jnp.bfloat16), before, preferred_element_type=jnp.float32)
    key_t = jnp.where(hit_t > 0.0, rank_t, -1.0).astype(jnp.bfloat16)
    gate_hi = gate_t.astype(jnp.bfloat16)
    gate_lo = (gate_t - gate_hi.astype(jnp.float32)).astype(jnp.bfloat16)

    table = jnp.concatenate([key_t, gate_hi, gate_lo], axis=1)
    tall_row = lax.broadcasted_iota(jnp.int32, (256, 128), 0)
    tall_lane = lax.broadcasted_iota(jnp.int32, (256, 128), 1)
    for part in range(4):
        d = ((part * 32 + tall_row // SLOT) * STRIDE) & 127
        z = (me[0] + (d >> 5)) & 3
        y = (me[1] + (d >> 3)) & 3
        x = (me[2] + (d >> 1)) & 3
        co = (me[3] + d) & 1
        spread = (z * 32 + y * 8 + x * 2 + co == tall_lane).astype(jnp.float32).astype(jnp.bfloat16)
        found = jnp.dot(spread, table, preferred_element_type=jnp.float32)
        on = found[:, :128] == (tall_row & (SLOT - 1)).astype(jnp.float32)
        at = pl.ds(part * 256, 256)
        pick[at, :] = jnp.where(on, 1.0, 0.0).astype(jnp.bfloat16)
        g_hi[at, :] = jnp.where(on, found[:, 128:256], 0.0).astype(jnp.bfloat16)
        g_lo[at, :] = jnp.where(on, found[:, 256:], 0.0).astype(jnp.bfloat16)

    def clear(i, c):
        ret[pl.ds(pl.multiple_of(i * 16, 16), 16), pl.ds(CAP, SLOT - CAP)] = jnp.zeros((16, SLOT - CAP, 2048), jnp.bfloat16)
        return c

    lax.fori_loop(0, 8, clear, 0)

    for h in range(2):
        wanted = (lax.broadcasted_iota(jnp.int32, (LEN, 128), 1) < 64) == (h == 0)
        vx[pl.ds(h * LEN, LEN), pl.ds(128, 128)] = jnp.where(wanted, 1.0, 0.0).astype(jnp.bfloat16)
    rkv[0] = skv[0]
    rq[0] = sq[0]
    others16 = pl.ds(1, N_SP - 1)

    def sp_all(src, dst, s, r):
        return pltpu.make_async_remote_copy(
            src_ref=src, dst_ref=dst, send_sem=s, recv_sem=r, device_id=(sp, dp), device_id_type=MESH)

    sp_all(skv.at[others16], rkv.at[others16], kvs_sem, kvr_sem).wait_send()
    lax.fori_loop(1, N_SP, send_q, 0)
    sp_all(skv.at[others16], rkv.at[others16], kvs_sem, kvr_sem).wait_recv()

    low_lane = lane < 64

    def lay(g, c):
        for i in range(4):
            k = g * 4 + i
            pair = rkv[k].astype(jnp.float32)
            flipped = jnp.transpose(pair)
            top, none = flipped[0:64], jnp.zeros((64, 128), jnp.float32)
            swapped = pltpu.roll(pair, 64, 1)
            at = pl.ds(pl.multiple_of(k * 128, 128), 128)
            at2 = pl.ds(pl.multiple_of(LEN + k * 128, 128), 128)
            kt[:, at] = jnp.concatenate([top, none], axis=0).astype(jnp.bfloat16)
            kt[:, at2] = jnp.concatenate([none, top], axis=0).astype(jnp.bfloat16)
            vx[at, pl.ds(0, 128)] = jnp.where(low_lane, swapped, 0.0).astype(jnp.bfloat16)
            vx[at2, pl.ds(0, 128)] = jnp.where(low_lane, 0.0, pair).astype(jnp.bfloat16)
        return c

    lax.fori_loop(0, N_SP // 4, lay, 0)
    own_rows = pl.ds(pl.multiple_of(sp * 128, 128), 128)

    def back_rows(k):
        return sp_copy(ao.at[k], rows.at[:, own_rows], k, -1, bs_sem, br_sem)

    def scores(b, target, peaks):
        q = rq[pl.ds(b * 2, 2)].reshape(256, 128)

        def part(at, peak):
            s = jnp.dot(q, kt[:, pl.ds(at, KEYS)], preferred_element_type=jnp.float32)
            target[:, pl.ds(at, KEYS)] = s
            for i in range(0, KEYS, 128):
                peak = s[:, i : i + 128] if peak is None else jnp.maximum(peak, s[:, i : i + 128])
            return peak

        return part

    sp_all(sq.at[1], rq.at[1], qs_sem, qr_sem.at[0]).wait_recv()
    opening = scores(0, s_even, peak_even)
    for h in range(2):
        peak = None
        for at in range(h * LEN, h * LEN + LEN, KEYS):
            peak = opening(at, peak)
        peak_even[:, pl.ds(h * 128, 128)] = peak

    def block(b, held, held_peak, following, following_peak):
        @pl.when(b < BLOCKS - 1)
        def _():
            two = pl.ds(b * 2 + 2, 2)
            sp_all(sq.at[two], rq.at[two], qs_sem, qr_sem.at[b + 1]).wait_recv()

        part = scores(jnp.minimum(b + 1, BLOCKS - 1), following, following_peak)
        o = None
        for h in range(2):
            top = jnp.max(held_peak[:, pl.ds(h * 128, 128)], axis=1, keepdims=True)
            peak = None
            for at in range(h * LEN, h * LEN + LEN, KEYS):
                peak = part(at, peak)
                p = jnp.exp2((held[:, pl.ds(at, KEYS)] - top) * EXP_SCALE).astype(jnp.bfloat16)
                d = jnp.dot(p, vx[pl.ds(at, KEYS), :], preferred_element_type=jnp.float32)
                o = d if o is None else o + d
            following_peak[:, pl.ds(h * 128, 128)] = peak
        a = (o[:, :128] / o[:, 128:]).astype(jnp.bfloat16)
        ao[pl.ds(b * 2, 2)] = a.reshape(2, 128, 128)

        @pl.when(b > 0)
        def _():
            back_rows(b * 2).start()

        back_rows(b * 2 + 1).start()

    def two_blocks(i, c):
        block(i * 2, s_even, peak_even, s_odd, peak_odd)
        block(i * 2 + 1, s_odd, peak_odd, s_even, peak_even)

        @pl.when(i == 1)
        def _():
            w_relay()

        return c

    lax.fori_loop(0, BLOCKS // 2, two_blocks, 0)
    rows[:, own_rows] = ao[0]
    sp_all(sq.at[others16], rq.at[others16], qs_sem, qr_sem.at[0]).wait_send()
    w_share(later)
    w_share(last)
    w_finish()
    back_all16 = sp_all(ao.at[others16], ao.at[others16], bs_sem, br_sem)
    back_all16.wait_send()
    back_all16.wait_recv()

    total = jnp.zeros((128, 1), jnp.float32)
    for n in range(4):
        cols = pl.ds(n * 512, 512)
        part = jnp.dot(rows[...], w[:, cols], preferred_element_type=jnp.float32)
        part = part + res_ref[:, cols].astype(jnp.float32)
        mixed[:, cols] = part
        total = total + jnp.sum(part * part, axis=1, keepdims=True)
    scale = lax.rsqrt(total / 2048.0 + norm_eps)
    normed[...] = (mixed[...] * scale * ngain_ref[...]).astype(jnp.bfloat16)

    def send_copy(k):
        return pltpu.make_async_remote_copy(
            src_ref=send.at[k, pl.ds(0, CAP)], dst_ref=recv.at[k, pl.ds(0, CAP)],
            send_sem=s_sem, recv_sem=r_sem.at[k // PER],
            device_id=shifted(me, k, 1), device_id_type=MESH)

    def send_block(first, count, sem):
        at = pl.ds(first, count)
        return pltpu.make_async_remote_copy(
            src_ref=send.at[at, pl.ds(0, CAP)], dst_ref=recv.at[at, pl.ds(0, CAP)],
            send_sem=s_sem, recv_sem=sem, device_id=(sp, dp), device_id_type=MESH)

    def pack(chunk, c):
        at = pl.ds(pl.multiple_of(chunk * 128, 128), 128)
        packed = jnp.dot(pick[at, :], normed[...], preferred_element_type=jnp.float32).astype(jnp.bfloat16)
        send[pl.ds(pl.multiple_of(chunk * 16, 16), 16)] = packed.reshape(16, SLOT, 2048)

        def start(i, c):
            send_copy((chunk - 1) * 16 + i).start()
            return c

        lax.fori_loop(jnp.where(chunk == 1, 1, 0), jnp.where(chunk == 0, 0, 16), start, 0)
        return c

    lax.fori_loop(0, 8, pack, 0)
    lax.fori_loop(112, 128, lambda k, c: (send_copy(k).start(), c)[1], 0)
    recv[0] = send[0]

    for c in loads[1:4]:
        c.wait()
    xs = normed[...]
    hidden = silu_mul(
        jnp.dot(xs, sg[...], preferred_element_type=jnp.float32),
        jnp.dot(xs, su[...], preferred_element_type=jnp.float32)).astype(jnp.bfloat16)
    for n in range(4):
        cols = pl.ds(n * 512, 512)
        mixed[:, cols] = mixed[:, cols] + jnp.dot(hidden, sd[:, cols], preferred_element_type=jnp.float32)

    for c in loads[4:]:
        c.wait()

    def back_copy(k):
        return pltpu.make_async_remote_copy(
            src_ref=fout.at[k, pl.ds(0, CAP)], dst_ref=ret.at[k, pl.ds(0, CAP)],
            send_sem=s2_sem, recv_sem=r2_sem,
            device_id=shifted(me, k, -1), device_id_type=MESH)

    def expert(g, c):
        first = g * PER
        lo = jnp.where(g == 0, 1, 0)

        @pl.when(g == 0)
        def _():
            send_block(1, PER - 1, r_sem.at[0]).wait_recv()

        @pl.when(g > 0)
        def _():
            send_block(pl.multiple_of(first, PER), PER, r_sem.at[g]).wait_recv()

        at = pl.ds(pl.multiple_of(first, PER), PER)
        x = recv[at].reshape(PER * SLOT, 2048)
        hid[...] = silu_mul(
            jnp.dot(x, eg[...], preferred_element_type=jnp.float32),
            jnp.dot(x, eu[...], preferred_element_type=jnp.float32)).astype(jnp.bfloat16)
        h = hid[...]
        for n in range(4):
            cols = pl.ds(n * 512, 512)
            o = jnp.dot(h, ed[:, cols], preferred_element_type=jnp.float32).astype(jnp.bfloat16)
            fout[at, :, cols] = o.reshape(PER, SLOT, 512)

        def reply(i, c):
            back_copy(first + i).start()
            return c

        lax.fori_loop(lo, PER, reply, 0)
        return c

    lax.fori_loop(0, GROUPS, expert, 0)

    ret[0, pl.ds(0, CAP)] = fout[0, pl.ds(0, CAP)]

    send_block(1, N_DEV - 1, r_sem.at[0]).wait_send()
    others = pl.ds(1, N_DEV - 1)
    back_all = pltpu.make_async_remote_copy(
        src_ref=fout.at[others, pl.ds(0, CAP)], dst_ref=ret.at[others, pl.ds(0, CAP)],
        send_sem=s2_sem, recv_sem=r2_sem, device_id=(sp, dp), device_id_type=MESH)
    back_all.wait_send()
    back_all.wait_recv()
    dims = (((0,), (0,)), ((), ()))
    for n in range(4):
        cols = pl.ds(n * 512, 512)
        r = ret[:, :, cols].reshape(N_DEV * SLOT, 512)
        routed = lax.dot_general(g_hi[...], r, dims, preferred_element_type=jnp.float32)
        routed = routed + lax.dot_general(g_lo[...], r, dims, preferred_element_type=jnp.float32)
        out_ref[:, cols] = (mixed[:, cols] + routed).astype(jnp.bfloat16)


def layer(*operands):
    bf, f32 = jnp.bfloat16, jnp.float32
    V, A = pl.BlockSpec(memory_space=pltpu.VMEM), pl.BlockSpec(memory_space=pl.ANY)
    S = pltpu.SemaphoreType.DMA
    M = pltpu.VMEM
    return pl.pallas_call(
        layer_kernel,
        out_shape=jax.ShapeDtypeStruct((128, 2048), bf),
        in_specs=[V, V, V, V, V, V, A, V, V, V, V, A, A, A, A, A, A],
        out_specs=V,
        scratch_shapes=[
            M((2048, 2048), bf),
            M((2048, 512), bf), M((2048, 512), bf), M((512, 2048), bf),
            M((2048, 512), bf), M((2048, 512), bf), M((512, 2048), bf),
            M((128, 2048), f32), M((128, 2048), bf),
            M((1024, 128), bf), M((1024, 128), bf), M((1024, 128), bf),
            M((128, SLOT, 2048), bf), M((128, SLOT, 2048), bf),
            M((128, SLOT, 2048), bf), M((128, SLOT, 2048), bf),
            M((PER * SLOT, 512), bf),
            M((LEN, 128), f32), M((N_SP, 128, 128), bf), M((N_SP, 128, 128), bf), M((N_SP, 128, 128), bf),
            M((N_SP, 128, 128), bf), M((128, 2 * LEN), bf), M((2 * LEN, 256), bf), M((N_SP, 128, 128), bf),
            M((128, 2048), bf), M((256, 2 * LEN), f32), M((256, 2 * LEN), f32), M((256, 256), f32), M((256, 256), f32),
            S((7,)), S, S((GROUPS,)), S, S, S, S, S, S((BLOCKS,)), S, S, S, S((14,)),
        ],
        compiler_params=pltpu.CompilerParams(collective_id=0, has_side_effects=True, vmem_limit_bytes=63 * 2**20),
        name="layer",
    )(*operands)


def per_device(
    residual, query, key_value, out_weight, norm_gain, query_gain, key_gain, route_ids, route_weights,
    shared_gate, shared_up, shared_down, expert_gate, expert_up, expert_down,
):
    cosine, sine = rope_tables()
    combined = layer(
        query[0], key_value[0], jnp.asarray(cosine), jnp.asarray(sine), query_gain[None, :], key_gain[None, :],
        out_weight, residual[0], norm_gain[None, :], route_ids[0].T, route_weights[0].T,
        shared_gate, shared_up, shared_down, expert_gate, expert_up, expert_down,
    )
    return combined[None]


def solution(mesh):
    in_specs = (
        P("dp", "sp", None),
        P("dp", "sp", None, None),
        P("dp", "sp", None, None),
        P(None, "dp"),
        P(),
        P(),
        P(),
        P("dp", "sp", None),
        P("dp", "sp", None),
        P(),
        P(),
        P(),
        P(("sp", "dp"), None, None),
        P(("sp", "dp"), None, None),
        P(("sp", "dp"), None, None),
    )
    out_specs = P("dp", "sp", None)
    return jax.shard_map(
        per_device, mesh=mesh, in_specs=in_specs, out_specs=out_specs, check_vma=False
    )
```

```python
import math
import jax
import jax.numpy as jnp
from jax import lax
from jax.experimental import pallas as pl
from jax.experimental.pallas import tpu as pltpu
import numpy as np
from jax.sharding import PartitionSpec as P

MESH = pl.DeviceIdType.MESH
N_DEV = 128
CAP = 6
SLOT = 8
GROUPS = 4
PER = N_DEV // GROUPS
norm_eps = 1e-06
rope_theta = 10000.0
routed_scale = 2.5
N_SP = 16
LEN = 2048
BLOCKS = 8
HEADS = 4
STRIDE = 91
KEYS = 512
EXP_SCALE = 0.125 * math.log2(math.e)


def digits(n):
    return n // 32, (n // 8) % 4, (n // 2) % 4, n % 2


def shifted(me_digits, k, sign):
    d = lax.rem(k * STRIDE, 128)
    out = []
    for m, v, size in zip(me_digits, digits(d), (4, 4, 4, 2)):
        out.append(lax.rem(m + sign * v + size, size))
    z, y, x, c = out
    return z * 4 + y, x * 2 + c


def silu_mul(g, u):
    return g / (1.0 + jnp.exp(-g)) * u


def sp_shifted(me, k, sign):
    d = lax.rem(k * 7, 16)
    z = lax.rem(me[0] + sign * (d // 4) + 4, 4)
    y = lax.rem(me[1] + sign * lax.rem(d, 4) + 4, 4)
    return z * 4 + y


def rope_tables():
    lanes = np.arange(128)
    theta = (np.float32(rope_theta) ** (-(2 * (lanes % 16)).astype(np.float32) / np.float32(32))).astype(np.float32)
    angles = np.arange(64, dtype=np.float32)[:, None] * theta[None, :]
    sign = np.where(lanes % 32 < 16, -1.0, 1.0)
    return np.cos(angles).astype(np.float32), (np.sin(angles) * sign).astype(np.float32)


def layer_kernel(
    q_hbm, kv_hbm, cos_ref, sin_ref, qg_ref, kg_ref,
    w_ref, res_hbm, ngain_ref, ids_ref, rw_ref, sg_ref, su_ref, sd_ref, eg_ref, eu_ref, ed_ref,
    out_ref,
    q_ref, kv_ref, res_ref, w, sg, su, sd, eg, eu, ed, mixed, normed, g_hi, g_lo, pick, send, recv, fout, ret, hid,
    wide, sq, skv, rq, rkv, kt, vx, ao, rows, s_even, s_odd, peak_even, peak_odd,
    ld_sem, s_sem, r_sem, s2_sem, r2_sem, kvs_sem, kvr_sem, qs_sem, qr_sem, bs_sem, br_sem, ws_sem, wr_sem,
):
    sp = lax.axis_index("sp")
    dp = lax.axis_index("dp")
    me = (sp // 4, lax.rem(sp, 4), dp // 2, lax.rem(dp, 2))

    own_cols = pl.ds(pl.multiple_of(dp * 256, 256), 256)
    loads = [
        pltpu.make_async_copy(a, b, ld_sem.at[i])
        for i, (a, b) in enumerate(
            [(kv_hbm, kv_ref), (q_hbm, q_ref), (w_ref, w.at[:, own_cols]), (res_hbm, res_ref), (sg_ref, sg), (su_ref, su), (sd_ref, sd), (eg_ref.at[0], eg), (eu_ref.at[0], eu), (ed_ref.at[0], ed)]
        )
    ]
    for c in loads:
        c.start()
    barrier = pltpu.get_barrier_semaphore()

    sp_of = [((me[0] + i // 4) & 3) * 4 + ((me[1] + i % 4) & 3) for i in range(N_SP)]
    dp_of = [((me[2] + i // 2) & 3) * 2 + ((me[3] + i % 2) & 1) for i in range(8)]
    for i in range(1, N_DEV):
        pl.semaphore_signal(barrier, inc=1, device_id=(sp_of[i // 8], dp_of[i % 8]), device_id_type=MESH)

    lane = lax.broadcasted_iota(jnp.int32, (128, 128), 1)
    row = lax.broadcasted_iota(jnp.int32, (128, 128), 0)

    lane1 = lax.broadcasted_iota(jnp.int32, (1, 128), 1)
    swap_up = (lane1 & 31) < 16

    def turned_gain(g):
        return jnp.where(swap_up, pltpu.roll(g, 112, 1), pltpu.roll(g, 16, 1))

    def both(g):
        return jnp.concatenate([g, g], axis=1)

    col_lane = (lane1 & 63) >= 32
    first = pl.ds(0, 64)
    second = pl.ds(64, 64)
    q_gain, k_gain = both(qg_ref[...]), both(kg_ref[...])
    q_gain8, k_gain8 = jnp.broadcast_to(q_gain, (8, 128)), jnp.broadcast_to(k_gain, (8, 128))
    q_turn, k_turn = turned_gain(q_gain8)[0:1], turned_gain(k_gain8)[0:1]

    def table(ref):
        top = jnp.where(col_lane, ref[...], ref[pl.ds(sp * 2, 1), :])
        bottom = jnp.where(col_lane, ref[...], ref[pl.ds(sp * 2 + 1, 1), :])
        return jnp.concatenate([top, bottom], axis=0)

    cosine, sine = table(cos_ref), table(sin_ref)
    ones_block = ((row >> 6) == (lane >> 6)).astype(jnp.float32).astype(jnp.bfloat16)
    turn = ((row ^ 16) == lane).astype(jnp.float32).astype(jnp.bfloat16)

    def prepared(x, cos_gain, sin_gain):
        xb = x.astype(jnp.bfloat16)
        square = x * x
        high = square.astype(jnp.bfloat16)
        low = (square - high.astype(jnp.float32)).astype(jnp.bfloat16)
        total = jnp.dot(high, ones_block, preferred_element_type=jnp.float32)
        total = total + jnp.dot(low, ones_block, preferred_element_type=jnp.float32)
        other = jnp.dot(xb, turn, preferred_element_type=jnp.float32)
        return lax.rsqrt(total / 64.0 + norm_eps) * (x * cos_gain + other * sin_gain)

    def prepare_all(source, target, cos_gain, sin_gain, keep):
        wide[...] = source[...].astype(jnp.float32).reshape(LEN, 128)

        def some(g, c):
            x = jnp.concatenate(
                [wide[pl.ds(sp_shifted(me, g * HEADS + i, 1), 128, stride=16), :] for i in range(HEADS)], axis=0)
            y = prepared(x, cos_gain, sin_gain)
            if keep:
                y = jnp.where(jnp.broadcast_to(lane1 < 64, y.shape), y, x)
            target[pl.ds(g * HEADS, HEADS)] = y.astype(jnp.bfloat16).reshape(HEADS, 128, 128)
            return c

        lax.fori_loop(0, N_SP // HEADS, some, 0)

    def stacked(t):
        return jnp.concatenate([t] * HEADS, axis=0)

    loads[0].wait()
    prepare_all(kv_ref, skv, stacked(cosine * k_gain), stacked(sine * k_turn), True)

    pl.semaphore_wait(barrier, N_DEV - 1)

    def sp_copy(src, dst, k, sign, s, r):
        return pltpu.make_async_remote_copy(
            src_ref=src, dst_ref=dst, send_sem=s, recv_sem=r,
            device_id=(sp_shifted(me, k, sign), dp), device_id_type=MESH)

    def send_kv(k, c):
        sp_copy(skv.at[k], rkv.at[k], k, 1, kvs_sem, kvr_sem).start()
        return c

    def send_q(k, c):
        sp_copy(sq.at[k], rq.at[k], k, 1, qs_sem, qr_sem.at[k // 2]).start()
        return c

    lax.fori_loop(1, N_SP, send_kv, 0)

    loads[2].wait()
    x_at, core = me[2], me[3]
    right, left, far = lax.rem(x_at + 1, 4), lax.rem(x_at + 3, 4), lax.rem(x_at + 2, 4)
    HALF, SUB = 512, 128

    def w_copy(first, size, x_from, device, number):
        at = w.at[pl.ds(first, size), pl.ds(pl.multiple_of((x_from * 2 + core) * 256, 256), 256)]
        return pltpu.make_async_remote_copy(
            src_ref=at, dst_ref=at, send_sem=ws_sem, recv_sem=wr_sem.at[number],
            device_id=device, device_id_type=MESH)

    def w_wait(rows, columns, number):
        at = w.at[pl.ds(0, rows), pl.ds(0, columns)]
        pltpu.make_async_remote_copy(
            src_ref=at, dst_ref=at, send_sem=ws_sem, recv_sem=wr_sem.at[number],
            device_id=(sp, dp), device_id_type=MESH).wait_recv()

    def along_x(x_to):
        return (sp, x_to * 2 + core)

    other_core = (sp, x_at * 2 + 1 - core)
    y_sub = pl.multiple_of(1024 + me[1] * SUB, SUB)
    z_sub = pl.multiple_of(1536 + me[0] * SUB, SUB)
    for x_to in (right, left, far):
        w_copy(y_sub, SUB, x_at, along_x(x_to), 0).start()
        w_copy(z_sub, SUB, x_at, along_x(x_to), 0).start()
    w_copy(0, HALF, x_at, along_x(right), 1).start()
    w_copy(HALF, HALF, x_at, along_x(left), 2).start()
    w_copy(HALF, HALF, x_at, along_x(right), 3).start()
    w_copy(0, HALF, x_at, along_x(left), 4).start()
    w_copy(0, LEN, x_at, other_core, 7).start()

    def y_sub_of(step):
        return pl.multiple_of(1024 + lax.rem(me[1] + step, 4) * SUB, SUB)

    def z_sub_of(step):
        return pl.multiple_of(1536 + lax.rem(me[0] + step, 4) * SUB, SUB)

    def w_lines():
        w_wait(6 * SUB, 256, 0)
        for step in range(1, 4):
            y_to, z_to = lax.rem(me[1] + step, 4), lax.rem(me[0] + step, 4)
            for x_from in (right, left, far):
                w_copy(y_sub, SUB, x_from, (me[0] * 4 + y_to, dp), 16 + step).start()
                w_copy(z_sub, SUB, x_from, (z_to * 4 + me[1], dp), 19 + step).start()
        for x_from in (right, left, far):
            w_copy(y_sub, SUB, x_from, other_core, 5).start()
            w_copy(z_sub, SUB, x_from, other_core, 5).start()

    def w_relay():
        w_wait(HALF, 256, 1)
        w_wait(HALF, 256, 2)
        w_copy(0, HALF, left, along_x(right), 8).start()
        w_copy(HALF, HALF, right, along_x(left), 9).start()
        w_copy(0, HALF, left, other_core, 10).start()
        w_copy(HALF, HALF, right, other_core, 11).start()

    def w_later():
        w_wait(HALF, 256, 3)
        w_wait(HALF, 256, 4)
        w_copy(HALF, HALF, left, other_core, 12).start()
        w_copy(0, HALF, right, other_core, 13).start()

    def w_finish():
        for step in range(1, 4):
            w_wait(3 * SUB, 256, 16 + step)
            for x_from in (right, left, far):
                w_copy(y_sub_of(4 - step), SUB, x_from, other_core, 14).start()
            w_wait(3 * SUB, 256, 19 + step)
            for x_from in (right, left, far):
                w_copy(z_sub_of(4 - step), SUB, x_from, other_core, 14).start()
        w_wait(HALF, 256, 8)
        w_copy(0, HALF, far, other_core, 15).start()
        w_wait(HALF, 256, 9)
        w_copy(HALF, HALF, far, other_core, 16).start()
        w_wait(LEN, 256, 7)
        for number in range(10, 14):
            w_wait(HALF, 256, number)
        w_wait(6 * SUB, 256, 5)
        w_wait(9 * SUB, 512, 14)
        w_wait(HALF, 256, 15)
        w_wait(HALF, 256, 16)

    def w_sent():
        everything = w.at[:, pl.ds(0, 7 * 256)]
        pltpu.make_async_remote_copy(
            src_ref=everything, dst_ref=everything, send_sem=ws_sem, recv_sem=wr_sem.at[0],
            device_id=(sp, dp), device_id_type=MESH).wait_send()

    loads[1].wait()
    prepare_all(q_ref, sq, stacked(cosine * q_gain), stacked(sine * q_turn), False)

    raw = rw_ref[...]
    gates = raw / jnp.sum(raw, axis=0, keepdims=True) * routed_scale
    ids = ids_ref[...]
    hit_t = jnp.zeros((128, 128), jnp.float32)
    gate_t = jnp.zeros((128, 128), jnp.float32)
    for j in range(4):
        on = ids[j : j + 1, :] == row
        hit_t = hit_t + jnp.where(on, 1.0, 0.0)
        gate_t = gate_t + jnp.where(on, gates[j : j + 1, :], 0.0)
    before = (row < lane).astype(jnp.float32).astype(jnp.bfloat16)
    rank_t = jnp.dot(hit_t.astype(jnp.bfloat16), before, preferred_element_type=jnp.float32)
    key_t = jnp.where(hit_t > 0.0, rank_t, -1.0).astype(jnp.bfloat16)
    gate_hi = gate_t.astype(jnp.bfloat16)
    gate_lo = (gate_t - gate_hi.astype(jnp.float32)).astype(jnp.bfloat16)

    table = jnp.concatenate([key_t, gate_hi, gate_lo], axis=1)
    tall_row = lax.broadcasted_iota(jnp.int32, (256, 128), 0)
    tall_lane = lax.broadcasted_iota(jnp.int32, (256, 128), 1)
    for part in range(4):
        d = ((part * 32 + tall_row // SLOT) * STRIDE) & 127
        z = (me[0] + (d >> 5)) & 3
        y = (me[1] + (d >> 3)) & 3
        x = (me[2] + (d >> 1)) & 3
        co = (me[3] + d) & 1
        spread = (z * 32 + y * 8 + x * 2 + co == tall_lane).astype(jnp.float32).astype(jnp.bfloat16)
        found = jnp.dot(spread, table, preferred_element_type=jnp.float32)
        on = found[:, :128] == (tall_row & (SLOT - 1)).astype(jnp.float32)
        at = pl.ds(part * 256, 256)
        pick[at, :] = jnp.where(on, 1.0, 0.0).astype(jnp.bfloat16)
        g_hi[at, :] = jnp.where(on, found[:, 128:256], 0.0).astype(jnp.bfloat16)
        g_lo[at, :] = jnp.where(on, found[:, 256:], 0.0).astype(jnp.bfloat16)

    def clear(i, c):
        ret[pl.ds(pl.multiple_of(i * 16, 16), 16), pl.ds(CAP, SLOT - CAP)] = jnp.zeros((16, SLOT - CAP, 2048), jnp.bfloat16)
        return c

    lax.fori_loop(0, 8, clear, 0)

    for h in range(2):
        wanted = (lax.broadcasted_iota(jnp.int32, (LEN, 128), 1) < 64) == (h == 0)
        vx[pl.ds(h * LEN, LEN), pl.ds(128, 128)] = jnp.where(wanted, 1.0, 0.0).astype(jnp.bfloat16)
    rkv[0] = skv[0]
    rq[0] = sq[0]
    others16 = pl.ds(1, N_SP - 1)

    def sp_all(src, dst, s, r):
        return pltpu.make_async_remote_copy(
            src_ref=src, dst_ref=dst, send_sem=s, recv_sem=r, device_id=(sp, dp), device_id_type=MESH)

    sp_all(skv.at[others16], rkv.at[others16], kvs_sem, kvr_sem).wait_send()
    lax.fori_loop(1, N_SP, send_q, 0)
    sp_all(skv.at[others16], rkv.at[others16], kvs_sem, kvr_sem).wait_recv()

    low_lane = lane < 64

    def lay(g, c):
        for i in range(4):
            k = g * 4 + i
            pair = rkv[k].astype(jnp.float32)
            flipped = jnp.transpose(pair)
            top, none = flipped[0:64], jnp.zeros((64, 128), jnp.float32)
            swapped = pltpu.roll(pair, 64, 1)
            at = pl.ds(pl.multiple_of(k * 128, 128), 128)
            at2 = pl.ds(pl.multiple_of(LEN + k * 128, 128), 128)
            kt[:, at] = jnp.concatenate([top, none], axis=0).astype(jnp.bfloat16)
            kt[:, at2] = jnp.concatenate([none, top], axis=0).astype(jnp.bfloat16)
            vx[at, pl.ds(0, 128)] = jnp.where(low_lane, swapped, 0.0).astype(jnp.bfloat16)
            vx[at2, pl.ds(0, 128)] = jnp.where(low_lane, 0.0, pair).astype(jnp.bfloat16)
        return c

    lax.fori_loop(0, N_SP // 4, lay, 0)
    own_rows = pl.ds(pl.multiple_of(sp * 128, 128), 128)

    def back_rows(k):
        return sp_copy(ao.at[k], rows.at[:, own_rows], k, -1, bs_sem, br_sem)

    def scores(b, target, peaks):
        q = rq[pl.ds(b * 2, 2)].reshape(256, 128)

        def part(at, peak):
            s = jnp.dot(q, kt[:, pl.ds(at, KEYS)], preferred_element_type=jnp.float32)
            target[:, pl.ds(at, KEYS)] = s
            for i in range(0, KEYS, 128):
                peak = s[:, i : i + 128] if peak is None else jnp.maximum(peak, s[:, i : i + 128])
            return peak

        return part

    sp_all(sq.at[1], rq.at[1], qs_sem, qr_sem.at[0]).wait_recv()
    opening = scores(0, s_even, peak_even)
    for h in range(2):
        peak = None
        for at in range(h * LEN, h * LEN + LEN, KEYS):
            peak = opening(at, peak)
        peak_even[:, pl.ds(h * 128, 128)] = peak

    def block(b, held, held_peak, following, following_peak):
        @pl.when(b < BLOCKS - 1)
        def _():
            two = pl.ds(b * 2 + 2, 2)
            sp_all(sq.at[two], rq.at[two], qs_sem, qr_sem.at[b + 1]).wait_recv()

        part = scores(jnp.minimum(b + 1, BLOCKS - 1), following, following_peak)
        o = None
        for h in range(2):
            top = jnp.max(held_peak[:, pl.ds(h * 128, 128)], axis=1, keepdims=True)
            peak = None
            for at in range(h * LEN, h * LEN + LEN, KEYS):
                peak = part(at, peak)
                p = jnp.exp2((held[:, pl.ds(at, KEYS)] - top) * EXP_SCALE).astype(jnp.bfloat16)
                d = jnp.dot(p, vx[pl.ds(at, KEYS), :], preferred_element_type=jnp.float32)
                o = d if o is None else o + d
            following_peak[:, pl.ds(h * 128, 128)] = peak
        a = (o[:, :128] / o[:, 128:]).astype(jnp.bfloat16)
        ao[pl.ds(b * 2, 2)] = a.reshape(2, 128, 128)

        @pl.when(b > 0)
        def _():
            back_rows(b * 2).start()

        back_rows(b * 2 + 1).start()

    def two_blocks(i, c):
        block(i * 2, s_even, peak_even, s_odd, peak_odd)
        @pl.when(i == 0)
        def _():
            w_lines()

        block(i * 2 + 1, s_odd, peak_odd, s_even, peak_even)

        @pl.when(i == 1)
        def _():
            w_relay()

        @pl.when(i == 2)
        def _():
            w_later()

        return c

    lax.fori_loop(0, BLOCKS // 2, two_blocks, 0)
    rows[:, own_rows] = ao[0]
    sp_all(sq.at[others16], rq.at[others16], qs_sem, qr_sem.at[0]).wait_send()
    w_finish()
    back_all16 = sp_all(ao.at[others16], ao.at[others16], bs_sem, br_sem)
    back_all16.wait_send()
    back_all16.wait_recv()

    loads[3].wait()
    total = jnp.zeros((128, 1), jnp.float32)
    for n in range(4):
        cols = pl.ds(n * 512, 512)
        part = jnp.dot(rows[...], w[:, cols], preferred_element_type=jnp.float32)
        part = part + res_ref[:, cols].astype(jnp.float32)
        mixed[:, cols] = part
        total = total + jnp.sum(part * part, axis=1, keepdims=True)
    scale = lax.rsqrt(total / 2048.0 + norm_eps)
    normed[...] = (mixed[...] * scale * ngain_ref[...]).astype(jnp.bfloat16)

    def send_copy(k):
        return pltpu.make_async_remote_copy(
            src_ref=send.at[k, pl.ds(0, CAP)], dst_ref=recv.at[k, pl.ds(0, CAP)],
            send_sem=s_sem, recv_sem=r_sem.at[k // PER],
            device_id=shifted(me, k, 1), device_id_type=MESH)

    def send_block(first, count, sem):
        at = pl.ds(first, count)
        return pltpu.make_async_remote_copy(
            src_ref=send.at[at, pl.ds(0, CAP)], dst_ref=recv.at[at, pl.ds(0, CAP)],
            send_sem=s_sem, recv_sem=sem, device_id=(sp, dp), device_id_type=MESH)

    def pack(chunk, c):
        at = pl.ds(pl.multiple_of(chunk * 128, 128), 128)
        packed = jnp.dot(pick[at, :], normed[...], preferred_element_type=jnp.float32).astype(jnp.bfloat16)
        send[pl.ds(pl.multiple_of(chunk * 16, 16), 16)] = packed.reshape(16, SLOT, 2048)

        def start(i, c):
            send_copy((chunk - 1) * 16 + i).start()
            return c

        lax.fori_loop(jnp.where(chunk == 1, 1, 0), jnp.where(chunk == 0, 0, 16), start, 0)
        return c

    lax.fori_loop(0, 8, pack, 0)
    lax.fori_loop(112, 128, lambda k, c: (send_copy(k).start(), c)[1], 0)
    recv[0] = send[0]

    for c in loads[4:7]:
        c.wait()
    xs = normed[...]
    hidden = silu_mul(
        jnp.dot(xs, sg[...], preferred_element_type=jnp.float32),
        jnp.dot(xs, su[...], preferred_element_type=jnp.float32)).astype(jnp.bfloat16)
    for n in range(4):
        cols = pl.ds(n * 512, 512)
        mixed[:, cols] = mixed[:, cols] + jnp.dot(hidden, sd[:, cols], preferred_element_type=jnp.float32)

    for c in loads[7:]:
        c.wait()

    def back_copy(k):
        return pltpu.make_async_remote_copy(
            src_ref=fout.at[k, pl.ds(0, CAP)], dst_ref=ret.at[k, pl.ds(0, CAP)],
            send_sem=s2_sem, recv_sem=r2_sem.at[k // PER],
            device_id=shifted(me, k, -1), device_id_type=MESH)

    def expert(g, c):
        first = g * PER
        lo = jnp.where(g == 0, 1, 0)

        @pl.when(g == 0)
        def _():
            send_block(1, PER - 1, r_sem.at[0]).wait_recv()

        @pl.when(g > 0)
        def _():
            send_block(pl.multiple_of(first, PER), PER, r_sem.at[g]).wait_recv()

        at = pl.ds(pl.multiple_of(first, PER), PER)
        x = recv[at].reshape(PER * SLOT, 2048)
        hid[...] = silu_mul(
            jnp.dot(x, eg[...], preferred_element_type=jnp.float32),
            jnp.dot(x, eu[...], preferred_element_type=jnp.float32)).astype(jnp.bfloat16)
        h = hid[...]
        for n in range(4):
            cols = pl.ds(n * 512, 512)
            o = jnp.dot(h, ed[:, cols], preferred_element_type=jnp.float32).astype(jnp.bfloat16)
            fout[at, :, cols] = o.reshape(PER, SLOT, 512)

        def reply(i, c):
            back_copy(first + i).start()
            return c

        lax.fori_loop(lo, PER, reply, 0)
        return c

    lax.fori_loop(0, GROUPS, expert, 0)

    ret[0, pl.ds(0, CAP)] = fout[0, pl.ds(0, CAP)]

    def back_block(first, count, number):
        at = pl.ds(first, count)
        return pltpu.make_async_remote_copy(
            src_ref=fout.at[at, pl.ds(0, CAP)], dst_ref=ret.at[at, pl.ds(0, CAP)],
            send_sem=s2_sem, recv_sem=r2_sem.at[number], device_id=(sp, dp), device_id_type=MESH)

    w_sent()
    send_block(1, N_DEV - 1, r_sem.at[0]).wait_send()
    dims = (((0,), (0,)), ((), ()))
    for g in range(GROUPS):
        first = max(1, g * PER)
        back_block(first, (g + 1) * PER - first, g).wait_recv()
        at = pl.ds(g * PER * SLOT, PER * SLOT)
        for n in range(4):
            cols = pl.ds(n * 512, 512)
            r = ret[pl.ds(g * PER, PER), :, cols].reshape(PER * SLOT, 512)
            routed = lax.dot_general(g_hi[at, :], r, dims, preferred_element_type=jnp.float32)
            routed = routed + lax.dot_general(g_lo[at, :], r, dims, preferred_element_type=jnp.float32)
            if g < GROUPS - 1:
                mixed[:, cols] = mixed[:, cols] + routed
            else:
                out_ref[:, cols] = (mixed[:, cols] + routed).astype(jnp.bfloat16)
    back_block(1, N_DEV - 1, 0).wait_send()


def layer(*operands):
    bf, f32 = jnp.bfloat16, jnp.float32
    V, A = pl.BlockSpec(memory_space=pltpu.VMEM), pl.BlockSpec(memory_space=pl.ANY)
    S = pltpu.SemaphoreType.DMA
    M = pltpu.VMEM
    return pl.pallas_call(
        layer_kernel,
        out_shape=jax.ShapeDtypeStruct((128, 2048), bf),
        in_specs=[A, A, V, V, V, V, A, A, V, V, V, A, A, A, A, A, A],
        out_specs=V,
        scratch_shapes=[
            M((128, 16, 128), bf), M((128, 16, 128), bf), M((128, 2048), bf),
            M((2048, 2048), bf),
            M((2048, 512), bf), M((2048, 512), bf), M((512, 2048), bf),
            M((2048, 512), bf), M((2048, 512), bf), M((512, 2048), bf),
            M((128, 2048), f32), M((128, 2048), bf),
            M((1024, 128), bf), M((1024, 128), bf), M((1024, 128), bf),
            M((128, SLOT, 2048), bf), M((128, SLOT, 2048), bf),
            M((128, SLOT, 2048), bf), M((128, SLOT, 2048), bf),
            M((PER * SLOT, 512), bf),
            M((LEN, 128), f32), M((N_SP, 128, 128), bf), M((N_SP, 128, 128), bf), M((N_SP, 128, 128), bf),
            M((N_SP, 128, 128), bf), M((128, 2 * LEN), bf), M((2 * LEN, 256), bf), M((N_SP, 128, 128), bf),
            M((128, 2048), bf), M((256, 2 * LEN), f32), M((256, 2 * LEN), f32), M((256, 256), f32), M((256, 256), f32),
            S((10,)), S, S((GROUPS,)), S, S((GROUPS,)), S, S, S, S((BLOCKS,)), S, S, S, S((23,)),
        ],
        compiler_params=pltpu.CompilerParams(collective_id=0, has_side_effects=True, vmem_limit_bytes=63 * 2**20),
        name="layer",
    )(*operands)


def per_device(
    residual, query, key_value, out_weight, norm_gain, query_gain, key_gain, route_ids, route_weights,
    shared_gate, shared_up, shared_down, expert_gate, expert_up, expert_down,
):
    cosine, sine = rope_tables()
    combined = layer(
        query[0], key_value[0], jnp.asarray(cosine), jnp.asarray(sine), query_gain[None, :], key_gain[None, :],
        out_weight, residual[0], norm_gain[None, :], route_ids[0].T, route_weights[0].T,
        shared_gate, shared_up, shared_down, expert_gate, expert_up, expert_down,
    )
    return combined[None]


def solution(mesh):
    in_specs = (
        P("dp", "sp", None),
        P("dp", "sp", None, None),
        P("dp", "sp", None, None),
        P(None, "dp"),
        P(),
        P(),
        P(),
        P("dp", "sp", None),
        P("dp", "sp", None),
        P(),
        P(),
        P(),
        P(("sp", "dp"), None, None),
        P(("sp", "dp"), None, None),
        P(("sp", "dp"), None, None),
    )
    out_specs = P("dp", "sp", None)
    return jax.shard_map(
        per_device, mesh=mesh, in_specs=in_specs, out_specs=out_specs, check_vma=False
    )
```

```python
import math
import jax
import jax.numpy as jnp
from jax import lax
from jax.experimental import pallas as pl
from jax.experimental.pallas import tpu as pltpu
import numpy as np
from jax.sharding import PartitionSpec as P

MESH = pl.DeviceIdType.MESH
N_DEV = 128
CAP = 6
SLOT = 8
GROUPS = 4
PER = N_DEV // GROUPS
norm_eps = 1e-06
rope_theta = 10000.0
routed_scale = 2.5
N_SP = 16
LEN = 2048
BLOCKS = 8
HEADS = 4
STRIDE = 91
KEYS = 512
EXP_SCALE = 0.125 * math.log2(math.e)


def digits(n):
    return n // 32, (n // 8) % 4, (n // 2) % 4, n % 2


def shifted(me_digits, k, sign):
    d = lax.rem(k * STRIDE, 128)
    out = []
    for m, v, size in zip(me_digits, digits(d), (4, 4, 4, 2)):
        out.append(lax.rem(m + sign * v + size, size))
    z, y, x, c = out
    return z * 4 + y, x * 2 + c


def silu_mul(g, u):
    return g / (1.0 + jnp.exp(-g)) * u


def sp_shifted(me, k, sign):
    d = lax.rem(k * 7, 16)
    z = lax.rem(me[0] + sign * (d // 4) + 4, 4)
    y = lax.rem(me[1] + sign * lax.rem(d, 4) + 4, 4)
    return z * 4 + y


def rope_tables():
    lanes = np.arange(128)
    theta = (np.float32(rope_theta) ** (-(2 * (lanes % 16)).astype(np.float32) / np.float32(32))).astype(np.float32)
    angles = np.arange(64, dtype=np.float32)[:, None] * theta[None, :]
    sign = np.where(lanes % 32 < 16, -1.0, 1.0)
    return np.cos(angles).astype(np.float32), (np.sin(angles) * sign).astype(np.float32)


def layer_kernel(
    q_hbm, kv_hbm, cos_ref, sin_ref, qg_ref, kg_ref,
    w_ref, res_hbm, ngain_ref, ids_ref, rw_ref, sg_ref, su_ref, sd_ref, eg_ref, eu_ref, ed_ref,
    out_ref,
    q_ref, kv_ref, res_ref, w, sg, su, sd, eg, eu, ed, mixed, normed, g_hi, g_lo, pick, send, recv, fout, ret, hid,
    wide, sq, skv, rq, rkv, kt, vx, ao, rows, s_even, s_odd, peak_even, peak_odd,
    ld_sem, s_sem, r_sem, s2_sem, r2_sem, kvs_sem, kvr_sem, qs_sem, qr_sem, bs_sem, br_sem, ws_sem, wr_sem, all_sem,
):
    sp = lax.axis_index("sp")
    dp = lax.axis_index("dp")
    me = (sp // 4, lax.rem(sp, 4), dp // 2, lax.rem(dp, 2))

    own_cols = pl.ds(pl.multiple_of(dp * 256, 256), 256)
    loads = [
        pltpu.make_async_copy(a, b, ld_sem.at[i])
        for i, (a, b) in enumerate(
            [(kv_hbm, kv_ref), (q_hbm, q_ref), (w_ref, w.at[:, own_cols]), (res_hbm, res_ref), (sg_ref, sg), (su_ref, su), (sd_ref, sd), (eg_ref.at[0], eg), (eu_ref.at[0], eu), (ed_ref.at[0], ed)]
        )
    ]
    for c in loads[:3]:
        c.start()
    barrier = pltpu.get_barrier_semaphore()

    sp_of = [((me[0] + i // 4) & 3) * 4 + ((me[1] + i % 4) & 3) for i in range(N_SP)]
    dp_of = [((me[2] + i // 2) & 3) * 2 + ((me[3] + i % 2) & 1) for i in range(8)]
    for i in range(1, N_SP):
        pl.semaphore_signal(barrier, inc=1, device_id=(sp_of[i], dp), device_id_type=MESH)
    for i in range(1, 8):
        pl.semaphore_signal(barrier, inc=1, device_id=(sp, dp_of[i]), device_id_type=MESH)

    lane = lax.broadcasted_iota(jnp.int32, (128, 128), 1)
    row = lax.broadcasted_iota(jnp.int32, (128, 128), 0)

    lane1 = lax.broadcasted_iota(jnp.int32, (1, 128), 1)
    swap_up = (lane1 & 31) < 16

    def turned_gain(g):
        return jnp.where(swap_up, pltpu.roll(g, 112, 1), pltpu.roll(g, 16, 1))

    def both(g):
        return jnp.concatenate([g, g], axis=1)

    col_lane = (lane1 & 63) >= 32
    first = pl.ds(0, 64)
    second = pl.ds(64, 64)
    q_gain, k_gain = both(qg_ref[...]), both(kg_ref[...])
    q_gain8, k_gain8 = jnp.broadcast_to(q_gain, (8, 128)), jnp.broadcast_to(k_gain, (8, 128))
    q_turn, k_turn = turned_gain(q_gain8)[0:1], turned_gain(k_gain8)[0:1]

    def table(ref):
        top = jnp.where(col_lane, ref[...], ref[pl.ds(sp * 2, 1), :])
        bottom = jnp.where(col_lane, ref[...], ref[pl.ds(sp * 2 + 1, 1), :])
        return jnp.concatenate([top, bottom], axis=0)

    cosine, sine = table(cos_ref), table(sin_ref)
    ones_block = ((row >> 6) == (lane >> 6)).astype(jnp.float32).astype(jnp.bfloat16)
    turn = ((row ^ 16) == lane).astype(jnp.float32).astype(jnp.bfloat16)

    def prepared(x, cos_gain, sin_gain):
        xb = x.astype(jnp.bfloat16)
        square = x * x
        high = square.astype(jnp.bfloat16)
        low = (square - high.astype(jnp.float32)).astype(jnp.bfloat16)
        total = jnp.dot(high, ones_block, preferred_element_type=jnp.float32)
        total = total + jnp.dot(low, ones_block, preferred_element_type=jnp.float32)
        other = jnp.dot(xb, turn, preferred_element_type=jnp.float32)
        return lax.rsqrt(total / 64.0 + norm_eps) * (x * cos_gain + other * sin_gain)

    def prepare_all(source, target, cos_gain, sin_gain, keep):
        wide[...] = source[...].astype(jnp.float32).reshape(LEN, 128)

        def some(g, c):
            x = jnp.concatenate(
                [wide[pl.ds(sp_shifted(me, g * HEADS + i, 1), 128, stride=16), :] for i in range(HEADS)], axis=0)
            y = prepared(x, cos_gain, sin_gain)
            if keep:
                y = jnp.where(jnp.broadcast_to(lane1 < 64, y.shape), y, x)
            target[pl.ds(g * HEADS, HEADS)] = y.astype(jnp.bfloat16).reshape(HEADS, 128, 128)
            return c

        lax.fori_loop(0, N_SP // HEADS, some, 0)

    def stacked(t):
        return jnp.concatenate([t] * HEADS, axis=0)

    loads[0].wait()
    prepare_all(kv_ref, skv, stacked(cosine * k_gain), stacked(sine * k_turn), True)

    pl.semaphore_wait(barrier, N_SP - 1 + 7)
    for i in range(1, 8):
        pl.semaphore_signal(all_sem, inc=1, device_id=(sp, dp_of[i]), device_id_type=MESH)

    def sp_copy(src, dst, k, sign, s, r):
        return pltpu.make_async_remote_copy(
            src_ref=src, dst_ref=dst, send_sem=s, recv_sem=r,
            device_id=(sp_shifted(me, k, sign), dp), device_id_type=MESH)

    def send_kv(k, c):
        sp_copy(skv.at[k], rkv.at[k], k, 1, kvs_sem, kvr_sem).start()
        return c

    def send_q(k, c):
        sp_copy(sq.at[k], rq.at[k], k, 1, qs_sem, qr_sem.at[k // 2]).start()
        return c

    lax.fori_loop(1, N_SP, send_kv, 0)

    loads[2].wait()
    x_at, core = me[2], me[3]
    right, left, far = lax.rem(x_at + 1, 4), lax.rem(x_at + 3, 4), lax.rem(x_at + 2, 4)
    HALF, SUB = 576, 112
    Y_ROWS, Z_ROWS = 2 * HALF, 2 * HALF + 4 * SUB

    def w_copy(first, size, x_from, device, number):
        at = w.at[pl.ds(first, size), pl.ds(pl.multiple_of((x_from * 2 + core) * 256, 256), 256)]
        return pltpu.make_async_remote_copy(
            src_ref=at, dst_ref=at, send_sem=ws_sem, recv_sem=wr_sem.at[number],
            device_id=device, device_id_type=MESH)

    def w_wait(rows, columns, number):
        at = w.at[pl.ds(0, rows), pl.ds(0, columns)]
        pltpu.make_async_remote_copy(
            src_ref=at, dst_ref=at, send_sem=ws_sem, recv_sem=wr_sem.at[number],
            device_id=(sp, dp), device_id_type=MESH).wait_recv()

    def along_x(x_to):
        return (sp, x_to * 2 + core)

    other_core = (sp, x_at * 2 + 1 - core)
    y_sub = pl.multiple_of(Y_ROWS + me[1] * SUB, 16)
    z_sub = pl.multiple_of(Z_ROWS + me[0] * SUB, 16)
    for x_to in (right, left, far):
        w_copy(y_sub, SUB, x_at, along_x(x_to), 0).start()
        w_copy(z_sub, SUB, x_at, along_x(x_to), 0).start()
    w_copy(0, HALF, x_at, along_x(right), 1).start()
    w_copy(HALF, HALF, x_at, along_x(left), 2).start()
    w_copy(HALF, HALF, x_at, along_x(right), 3).start()
    w_copy(0, HALF, x_at, along_x(left), 4).start()
    w_copy(0, LEN, x_at, other_core, 7).start()
    for c in loads[3:]:
        c.start()

    def y_sub_of(step):
        return pl.multiple_of(Y_ROWS + lax.rem(me[1] + step, 4) * SUB, 16)

    def z_sub_of(step):
        return pl.multiple_of(Z_ROWS + lax.rem(me[0] + step, 4) * SUB, 16)

    def w_lines():
        w_wait(6 * SUB, 256, 0)
        for step in range(1, 4):
            y_to, z_to = lax.rem(me[1] + step, 4), lax.rem(me[0] + step, 4)
            for x_from in (right, left, far):
                w_copy(y_sub, SUB, x_from, (me[0] * 4 + y_to, dp), 16 + step).start()
                w_copy(z_sub, SUB, x_from, (z_to * 4 + me[1], dp), 19 + step).start()
        for x_from in (right, left, far):
            w_copy(y_sub, SUB, x_from, other_core, 5).start()
            w_copy(z_sub, SUB, x_from, other_core, 5).start()

    def w_relay():
        w_wait(HALF, 256, 1)
        w_wait(HALF, 256, 2)
        w_copy(0, HALF, left, along_x(right), 8).start()
        w_copy(HALF, HALF, right, along_x(left), 9).start()
        w_copy(0, HALF, left, other_core, 10).start()
        w_copy(HALF, HALF, right, other_core, 11).start()

    def w_later():
        w_wait(HALF, 256, 3)
        w_wait(HALF, 256, 4)
        w_copy(HALF, HALF, left, other_core, 12).start()
        w_copy(0, HALF, right, other_core, 13).start()

    def w_finish():
        for step in range(1, 4):
            w_wait(3 * SUB, 256, 16 + step)
            for x_from in (right, left, far):
                w_copy(y_sub_of(4 - step), SUB, x_from, other_core, 14).start()
            w_wait(3 * SUB, 256, 19 + step)
            for x_from in (right, left, far):
                w_copy(z_sub_of(4 - step), SUB, x_from, other_core, 14).start()
        w_wait(HALF, 256, 8)
        w_copy(0, HALF, far, other_core, 15).start()
        w_wait(HALF, 256, 9)
        w_copy(HALF, HALF, far, other_core, 16).start()
        w_wait(LEN, 256, 7)
        for number in range(10, 14):
            w_wait(HALF, 256, number)
        w_wait(6 * SUB, 256, 5)
        w_wait(9 * SUB, 512, 14)
        w_wait(HALF, 256, 15)
        w_wait(HALF, 256, 16)

    def w_sent():
        everything = w.at[:, pl.ds(0, 7 * 256)]
        pltpu.make_async_remote_copy(
            src_ref=everything, dst_ref=everything, send_sem=ws_sem, recv_sem=wr_sem.at[0],
            device_id=(sp, dp), device_id_type=MESH).wait_send()

    loads[1].wait()
    prepare_all(q_ref, sq, stacked(cosine * q_gain), stacked(sine * q_turn), False)

    raw = rw_ref[...]
    gates = raw / jnp.sum(raw, axis=0, keepdims=True) * routed_scale
    ids = ids_ref[...]
    hit_t = jnp.zeros((128, 128), jnp.float32)
    gate_t = jnp.zeros((128, 128), jnp.float32)
    for j in range(4):
        on = ids[j : j + 1, :] == row
        hit_t = hit_t + jnp.where(on, 1.0, 0.0)
        gate_t = gate_t + jnp.where(on, gates[j : j + 1, :], 0.0)
    before = (row < lane).astype(jnp.float32).astype(jnp.bfloat16)
    rank_t = jnp.dot(hit_t.astype(jnp.bfloat16), before, preferred_element_type=jnp.float32)
    key_t = jnp.where(hit_t > 0.0, rank_t, -1.0).astype(jnp.bfloat16)
    gate_hi = gate_t.astype(jnp.bfloat16)
    gate_lo = (gate_t - gate_hi.astype(jnp.float32)).astype(jnp.bfloat16)

    table = jnp.concatenate([key_t, gate_hi, gate_lo], axis=1)
    tall_row = lax.broadcasted_iota(jnp.int32, (256, 128), 0)
    tall_lane = lax.broadcasted_iota(jnp.int32, (256, 128), 1)
    for part in range(4):
        d = ((part * 32 + tall_row // SLOT) * STRIDE) & 127
        z = (me[0] + (d >> 5)) & 3
        y = (me[1] + (d >> 3)) & 3
        x = (me[2] + (d >> 1)) & 3
        co = (me[3] + d) & 1
        spread = (z * 32 + y * 8 + x * 2 + co == tall_lane).astype(jnp.float32).astype(jnp.bfloat16)
        found = jnp.dot(spread, table, preferred_element_type=jnp.float32)
        on = found[:, :128] == (tall_row & (SLOT - 1)).astype(jnp.float32)
        at = pl.ds(part * 256, 256)
        pick[at, :] = jnp.where(on, 1.0, 0.0).astype(jnp.bfloat16)
        g_hi[at, :] = jnp.where(on, found[:, 128:256], 0.0).astype(jnp.bfloat16)
        g_lo[at, :] = jnp.where(on, found[:, 256:], 0.0).astype(jnp.bfloat16)

    def clear(i, c):
        ret[pl.ds(pl.multiple_of(i * 16, 16), 16), pl.ds(CAP, SLOT - CAP)] = jnp.zeros((16, SLOT - CAP, 2048), jnp.bfloat16)
        return c

    lax.fori_loop(0, 8, clear, 0)

    for h in range(2):
        wanted = (lax.broadcasted_iota(jnp.int32, (LEN, 128), 1) < 64) == (h == 0)
        vx[pl.ds(h * LEN, LEN), pl.ds(128, 128)] = jnp.where(wanted, 1.0, 0.0).astype(jnp.bfloat16)
    rkv[0] = skv[0]
    rq[0] = sq[0]
    others16 = pl.ds(1, N_SP - 1)

    def sp_all(src, dst, s, r):
        return pltpu.make_async_remote_copy(
            src_ref=src, dst_ref=dst, send_sem=s, recv_sem=r, device_id=(sp, dp), device_id_type=MESH)

    sp_all(skv.at[others16], rkv.at[others16], kvs_sem, kvr_sem).wait_send()
    lax.fori_loop(1, N_SP, send_q, 0)
    sp_all(skv.at[others16], rkv.at[others16], kvs_sem, kvr_sem).wait_recv()

    low_lane = lane < 64

    def lay(g, c):
        for i in range(4):
            k = g * 4 + i
            pair = rkv[k].astype(jnp.float32)
            flipped = jnp.transpose(pair)
            top, none = flipped[0:64], jnp.zeros((64, 128), jnp.float32)
            swapped = pltpu.roll(pair, 64, 1)
            at = pl.ds(pl.multiple_of(k * 128, 128), 128)
            at2 = pl.ds(pl.multiple_of(LEN + k * 128, 128), 128)
            kt[:, at] = jnp.concatenate([top, none], axis=0).astype(jnp.bfloat16)
            kt[:, at2] = jnp.concatenate([none, top], axis=0).astype(jnp.bfloat16)
            vx[at, pl.ds(0, 128)] = jnp.where(low_lane, swapped, 0.0).astype(jnp.bfloat16)
            vx[at2, pl.ds(0, 128)] = jnp.where(low_lane, 0.0, pair).astype(jnp.bfloat16)
        return c

    lax.fori_loop(0, N_SP // 4, lay, 0)
    own_rows = pl.ds(pl.multiple_of(sp * 128, 128), 128)

    def back_rows(k):
        return sp_copy(ao.at[k], rows.at[:, own_rows], k, -1, bs_sem, br_sem)

    def scores(b, target, peaks):
        q = rq[pl.ds(b * 2, 2)].reshape(256, 128)

        def part(at, peak):
            s = jnp.dot(q, kt[:, pl.ds(at, KEYS)], preferred_element_type=jnp.float32)
            target[:, pl.ds(at, KEYS)] = s
            for i in range(0, KEYS, 128):
                peak = s[:, i : i + 128] if peak is None else jnp.maximum(peak, s[:, i : i + 128])
            return peak

        return part

    sp_all(sq.at[1], rq.at[1], qs_sem, qr_sem.at[0]).wait_recv()
    opening = scores(0, s_even, peak_even)
    for h in range(2):
        peak = None
        for at in range(h * LEN, h * LEN + LEN, KEYS):
            peak = opening(at, peak)
        peak_even[:, pl.ds(h * 128, 128)] = peak

    def block(b, held, held_peak, following, following_peak):
        @pl.when(b < BLOCKS - 1)
        def _():
            two = pl.ds(b * 2 + 2, 2)
            sp_all(sq.at[two], rq.at[two], qs_sem, qr_sem.at[b + 1]).wait_recv()

        part = scores(jnp.minimum(b + 1, BLOCKS - 1), following, following_peak)
        o = None
        for h in range(2):
            top = jnp.max(held_peak[:, pl.ds(h * 128, 128)], axis=1, keepdims=True)
            peak = None
            for at in range(h * LEN, h * LEN + LEN, KEYS):
                peak = part(at, peak)
                p = jnp.exp2((held[:, pl.ds(at, KEYS)] - top) * EXP_SCALE).astype(jnp.bfloat16)
                d = jnp.dot(p, vx[pl.ds(at, KEYS), :], preferred_element_type=jnp.float32)
                o = d if o is None else o + d
            following_peak[:, pl.ds(h * 128, 128)] = peak
        a = (o[:, :128] / o[:, 128:]).astype(jnp.bfloat16)
        ao[pl.ds(b * 2, 2)] = a.reshape(2, 128, 128)

        @pl.when(b > 0)
        def _():
            back_rows(b * 2).start()

        back_rows(b * 2 + 1).start()

    def two_blocks(i, c):
        block(i * 2, s_even, peak_even, s_odd, peak_odd)
        @pl.when(i == 0)
        def _():
            w_lines()

        block(i * 2 + 1, s_odd, peak_odd, s_even, peak_even)

        @pl.when(i == 1)
        def _():
            w_relay()

        @pl.when(i == 2)
        def _():
            w_later()

        return c

    lax.fori_loop(0, BLOCKS // 2, two_blocks, 0)
    rows[:, own_rows] = ao[0]
    sp_all(sq.at[others16], rq.at[others16], qs_sem, qr_sem.at[0]).wait_send()
    w_finish()
    back_all16 = sp_all(ao.at[others16], ao.at[others16], bs_sem, br_sem)
    back_all16.wait_send()
    back_all16.wait_recv()

    loads[3].wait()
    total = jnp.zeros((128, 1), jnp.float32)
    for n in range(4):
        cols = pl.ds(n * 512, 512)
        part = jnp.dot(rows[...], w[:, cols], preferred_element_type=jnp.float32)
        part = part + res_ref[:, cols].astype(jnp.float32)
        mixed[:, cols] = part
        total = total + jnp.sum(part * part, axis=1, keepdims=True)
    scale = lax.rsqrt(total / 2048.0 + norm_eps)
    normed[...] = (mixed[...] * scale * ngain_ref[...]).astype(jnp.bfloat16)

    pl.semaphore_wait(all_sem, 7)

    def send_copy(k):
        return pltpu.make_async_remote_copy(
            src_ref=send.at[k, pl.ds(0, CAP)], dst_ref=recv.at[k, pl.ds(0, CAP)],
            send_sem=s_sem, recv_sem=r_sem.at[k // PER],
            device_id=shifted(me, k, 1), device_id_type=MESH)

    def send_block(first, count, sem):
        at = pl.ds(first, count)
        return pltpu.make_async_remote_copy(
            src_ref=send.at[at, pl.ds(0, CAP)], dst_ref=recv.at[at, pl.ds(0, CAP)],
            send_sem=s_sem, recv_sem=sem, device_id=(sp, dp), device_id_type=MESH)

    def pack(chunk, c):
        at = pl.ds(pl.multiple_of(chunk * 128, 128), 128)
        packed = jnp.dot(pick[at, :], normed[...], preferred_element_type=jnp.float32).astype(jnp.bfloat16)
        send[pl.ds(pl.multiple_of(chunk * 16, 16), 16)] = packed.reshape(16, SLOT, 2048)

        def start(i, c):
            send_copy((chunk - 1) * 16 + i).start()
            return c

        lax.fori_loop(jnp.where(chunk == 1, 1, 0), jnp.where(chunk == 0, 0, 16), start, 0)
        return c

    lax.fori_loop(0, 8, pack, 0)
    lax.fori_loop(112, 128, lambda k, c: (send_copy(k).start(), c)[1], 0)
    recv[0] = send[0]

    for c in loads[4:7]:
        c.wait()
    xs = normed[...]
    hidden = silu_mul(
        jnp.dot(xs, sg[...], preferred_element_type=jnp.float32),
        jnp.dot(xs, su[...], preferred_element_type=jnp.float32)).astype(jnp.bfloat16)
    for n in range(4):
        cols = pl.ds(n * 512, 512)
        mixed[:, cols] = mixed[:, cols] + jnp.dot(hidden, sd[:, cols], preferred_element_type=jnp.float32)

    for c in loads[7:]:
        c.wait()

    def back_copy(k):
        return pltpu.make_async_remote_copy(
            src_ref=fout.at[k, pl.ds(0, CAP)], dst_ref=ret.at[k, pl.ds(0, CAP)],
            send_sem=s2_sem, recv_sem=r2_sem.at[k // PER],
            device_id=shifted(me, k, -1), device_id_type=MESH)

    def expert(g, c):
        first = g * PER
        lo = jnp.where(g == 0, 1, 0)

        @pl.when(g == 0)
        def _():
            send_block(1, PER - 1, r_sem.at[0]).wait_recv()

        @pl.when(g > 0)
        def _():
            send_block(pl.multiple_of(first, PER), PER, r_sem.at[g]).wait_recv()

        at = pl.ds(pl.multiple_of(first, PER), PER)
        x = recv[at].reshape(PER * SLOT, 2048)
        hid[...] = silu_mul(
            jnp.dot(x, eg[...], preferred_element_type=jnp.float32),
            jnp.dot(x, eu[...], preferred_element_type=jnp.float32)).astype(jnp.bfloat16)
        h = hid[...]
        for n in range(4):
            cols = pl.ds(n * 512, 512)
            o = jnp.dot(h, ed[:, cols], preferred_element_type=jnp.float32).astype(jnp.bfloat16)
            fout[at, :, cols] = o.reshape(PER, SLOT, 512)

        def reply(i, c):
            back_copy(first + i).start()
            return c

        lax.fori_loop(lo, PER, reply, 0)
        return c

    lax.fori_loop(0, GROUPS, expert, 0)

    ret[0, pl.ds(0, CAP)] = fout[0, pl.ds(0, CAP)]

    def back_block(first, count, number):
        at = pl.ds(first, count)
        return pltpu.make_async_remote_copy(
            src_ref=fout.at[at, pl.ds(0, CAP)], dst_ref=ret.at[at, pl.ds(0, CAP)],
            send_sem=s2_sem, recv_sem=r2_sem.at[number], device_id=(sp, dp), device_id_type=MESH)

    w_sent()
    send_block(1, N_DEV - 1, r_sem.at[0]).wait_send()
    dims = (((0,), (0,)), ((), ()))
    for g in range(GROUPS):
        first = max(1, g * PER)
        back_block(first, (g + 1) * PER - first, g).wait_recv()
        at = pl.ds(g * PER * SLOT, PER * SLOT)
        for n in range(4):
            cols = pl.ds(n * 512, 512)
            r = ret[pl.ds(g * PER, PER), :, cols].reshape(PER * SLOT, 512)
            routed = lax.dot_general(g_hi[at, :], r, dims, preferred_element_type=jnp.float32)
            routed = routed + lax.dot_general(g_lo[at, :], r, dims, preferred_element_type=jnp.float32)
            if g < GROUPS - 1:
                mixed[:, cols] = mixed[:, cols] + routed
            else:
                out_ref[:, cols] = (mixed[:, cols] + routed).astype(jnp.bfloat16)
    back_block(1, N_DEV - 1, 0).wait_send()


def layer(*operands):
    bf, f32 = jnp.bfloat16, jnp.float32
    V, A = pl.BlockSpec(memory_space=pltpu.VMEM), pl.BlockSpec(memory_space=pl.ANY)
    S = pltpu.SemaphoreType.DMA
    M = pltpu.VMEM
    return pl.pallas_call(
        layer_kernel,
        out_shape=pltpu.VMEM((128, 2048), bf),
        in_specs=[A, A, V, V, V, V, A, A, V, V, V, A, A, A, A, A, A],
        out_specs=V,
        scratch_shapes=[
            M((128, 16, 128), bf), M((128, 16, 128), bf), M((128, 2048), bf),
            M((2048, 2048), bf),
            M((2048, 512), bf), M((2048, 512), bf), M((512, 2048), bf),
            M((2048, 512), bf), M((2048, 512), bf), M((512, 2048), bf),
            M((128, 2048), f32), M((128, 2048), bf),
            M((1024, 128), bf), M((1024, 128), bf), M((1024, 128), bf),
            M((128, SLOT, 2048), bf), M((128, SLOT, 2048), bf),
            M((128, SLOT, 2048), bf), M((128, SLOT, 2048), bf),
            M((PER * SLOT, 512), bf),
            M((LEN, 128), f32), M((N_SP, 128, 128), bf), M((N_SP, 128, 128), bf), M((N_SP, 128, 128), bf),
            M((N_SP, 128, 128), bf), M((128, 2 * LEN), bf), M((2 * LEN, 256), bf), M((N_SP, 128, 128), bf),
            M((128, 2048), bf), M((256, 2 * LEN), f32), M((256, 2 * LEN), f32), M((256, 256), f32), M((256, 256), f32),
            S((10,)), S, S((GROUPS,)), S, S((GROUPS,)), S, S, S, S((BLOCKS,)), S, S, S, S((23,)), pltpu.SemaphoreType.REGULAR,
        ],
        compiler_params=pltpu.CompilerParams(collective_id=0, has_side_effects=True, vmem_limit_bytes=63 * 2**20),
        name="layer",
    )(*operands)


def per_device(
    residual, query, key_value, out_weight, norm_gain, query_gain, key_gain, route_ids, route_weights,
    shared_gate, shared_up, shared_down, expert_gate, expert_up, expert_down,
):
    cosine, sine = rope_tables()
    combined = layer(
        query[0], key_value[0], jnp.asarray(cosine), jnp.asarray(sine), query_gain[None, :], key_gain[None, :],
        out_weight, residual[0], norm_gain[None, :], route_ids[0].T, route_weights[0].T,
        shared_gate, shared_up, shared_down, expert_gate, expert_up, expert_down,
    )
    return combined[None]


def solution(mesh):
    in_specs = (
        P("dp", "sp", None),
        P("dp", "sp", None, None),
        P("dp", "sp", None, None),
        P(None, "dp"),
        P(),
        P(),
        P(),
        P("dp", "sp", None),
        P("dp", "sp", None),
        P(),
        P(),
        P(),
        P(("sp", "dp"), None, None),
        P(("sp", "dp"), None, None),
        P(("sp", "dp"), None, None),
    )
    out_specs = P("dp", "sp", None)
    return jax.shard_map(
        per_device, mesh=mesh, in_specs=in_specs, out_specs=out_specs, check_vma=False
    )
```

```python
import math
import jax
import jax.numpy as jnp
from jax import lax
from jax.experimental import pallas as pl
from jax.experimental.pallas import tpu as pltpu
import numpy as np
from jax.sharding import PartitionSpec as P

MESH = pl.DeviceIdType.MESH
N_DEV = 128
CAP = 6
SLOT = 8
GROUPS = 4
PER = N_DEV // GROUPS
norm_eps = 1e-06
rope_theta = 10000.0
routed_scale = 2.5
N_SP = 16
LEN = 2048
BLOCKS = 8
HEADS = 4
STRIDE = 101
KEYS = 512
EXP_SCALE = 0.125 * math.log2(math.e)


def digits(n):
    return n // 32, (n // 8) % 4, (n // 2) % 4, n % 2


def shifted(me_digits, k, sign):
    d = lax.rem(k * STRIDE, 128)
    out = []
    for m, v, size in zip(me_digits, digits(d), (4, 4, 4, 2)):
        out.append(lax.rem(m + sign * v + size, size))
    z, y, x, c = out
    return z * 4 + y, x * 2 + c


def silu_mul(g, u):
    return g / (1.0 + jnp.exp(-g)) * u


def sp_shifted(me, k, sign):
    d = lax.rem(k * 7, 16)
    z = lax.rem(me[0] + sign * (d // 4) + 4, 4)
    y = lax.rem(me[1] + sign * lax.rem(d, 4) + 4, 4)
    return z * 4 + y


def rope_tables():
    lanes = np.arange(128)
    theta = (np.float32(rope_theta) ** (-(2 * (lanes % 16)).astype(np.float32) / np.float32(32))).astype(np.float32)
    angles = np.arange(64, dtype=np.float32)[:, None] * theta[None, :]
    sign = np.where(lanes % 32 < 16, -1.0, 1.0)
    return np.cos(angles).astype(np.float32), (np.sin(angles) * sign).astype(np.float32)


def layer_kernel(
    q_hbm, kv_hbm, cos_ref, sin_ref, qg_ref, kg_ref,
    w_ref, res_hbm, ngain_ref, ids_ref, rw_ref, sg_ref, su_ref, sd_ref, eg_ref, eu_ref, ed_ref,
    out_ref,
    q_ref, kv_ref, res_ref, w, sg, su, sd, eg, eu, ed, mixed, normed, g_hi, g_lo, pick, send, recv, fout, ret, hid,
    wide, sq, skv, rq, rkv, kt, vx, ao, rows, s_even, s_odd, peak_even, peak_odd,
    ld_sem, s_sem, r_sem, s2_sem, r2_sem, kvs_sem, kvr_sem, qs_sem, qr_sem, bs_sem, br_sem, ws_sem, wr_sem, all_sem,
):
    sp = lax.axis_index("sp")
    dp = lax.axis_index("dp")
    me = (sp // 4, lax.rem(sp, 4), dp // 2, lax.rem(dp, 2))

    own_cols = pl.ds(pl.multiple_of(dp * 256, 256), 256)
    loads = [
        pltpu.make_async_copy(a, b, ld_sem.at[i])
        for i, (a, b) in enumerate(
            [(kv_hbm, kv_ref), (q_hbm, q_ref), (w_ref, w.at[:, own_cols]), (res_hbm, res_ref), (sg_ref, sg), (su_ref, su), (sd_ref, sd), (eg_ref.at[0], eg), (eu_ref.at[0], eu), (ed_ref.at[0], ed)]
        )
    ]
    for c in loads[:3]:
        c.start()
    barrier = pltpu.get_barrier_semaphore()

    sp_of = [((me[0] + i // 4) & 3) * 4 + ((me[1] + i % 4) & 3) for i in range(N_SP)]
    dp_of = [((me[2] + i // 2) & 3) * 2 + ((me[3] + i % 2) & 1) for i in range(8)]
    for i in range(1, N_SP):
        pl.semaphore_signal(barrier, inc=1, device_id=(sp_of[i], dp), device_id_type=MESH)
    for i in range(1, 8):
        pl.semaphore_signal(barrier, inc=1, device_id=(sp, dp_of[i]), device_id_type=MESH)

    lane = lax.broadcasted_iota(jnp.int32, (128, 128), 1)
    row = lax.broadcasted_iota(jnp.int32, (128, 128), 0)

    lane1 = lax.broadcasted_iota(jnp.int32, (1, 128), 1)
    swap_up = (lane1 & 31) < 16

    def turned_gain(g):
        return jnp.where(swap_up, pltpu.roll(g, 112, 1), pltpu.roll(g, 16, 1))

    def both(g):
        return jnp.concatenate([g, g], axis=1)

    col_lane = (lane1 & 63) >= 32
    first = pl.ds(0, 64)
    second = pl.ds(64, 64)
    q_gain, k_gain = both(qg_ref[...]), both(kg_ref[...])
    q_gain8, k_gain8 = jnp.broadcast_to(q_gain, (8, 128)), jnp.broadcast_to(k_gain, (8, 128))
    q_turn, k_turn = turned_gain(q_gain8)[0:1], turned_gain(k_gain8)[0:1]

    def table(ref):
        top = jnp.where(col_lane, ref[...], ref[pl.ds(sp * 2, 1), :])
        bottom = jnp.where(col_lane, ref[...], ref[pl.ds(sp * 2 + 1, 1), :])
        return jnp.concatenate([top, bottom], axis=0)

    cosine, sine = table(cos_ref), table(sin_ref)
    ones_block = ((row >> 6) == (lane >> 6)).astype(jnp.float32).astype(jnp.bfloat16)
    turn = ((row ^ 16) == lane).astype(jnp.float32).astype(jnp.bfloat16)

    def prepared(x, cos_gain, sin_gain):
        xb = x.astype(jnp.bfloat16)
        square = x * x
        high = square.astype(jnp.bfloat16)
        low = (square - high.astype(jnp.float32)).astype(jnp.bfloat16)
        total = jnp.dot(high, ones_block, preferred_element_type=jnp.float32)
        total = total + jnp.dot(low, ones_block, preferred_element_type=jnp.float32)
        other = jnp.dot(xb, turn, preferred_element_type=jnp.float32)
        return lax.rsqrt(total / 64.0 + norm_eps) * (x * cos_gain + other * sin_gain)

    def prepare_all(source, target, cos_gain, sin_gain, keep):
        wide[...] = source[...].astype(jnp.float32).reshape(LEN, 128)

        def some(g, c):
            x = jnp.concatenate(
                [wide[pl.ds(sp_shifted(me, g * HEADS + i, 1), 128, stride=16), :] for i in range(HEADS)], axis=0)
            y = prepared(x, cos_gain, sin_gain)
            if keep:
                y = jnp.where(jnp.broadcast_to(lane1 < 64, y.shape), y, x)
            target[pl.ds(g * HEADS, HEADS)] = y.astype(jnp.bfloat16).reshape(HEADS, 128, 128)
            return c

        lax.fori_loop(0, N_SP // HEADS, some, 0)

    def stacked(t):
        return jnp.concatenate([t] * HEADS, axis=0)

    loads[0].wait()
    prepare_all(kv_ref, skv, stacked(cosine * k_gain), stacked(sine * k_turn), True)

    pl.semaphore_wait(barrier, N_SP - 1 + 7)
    for i in range(1, 8):
        pl.semaphore_signal(all_sem, inc=1, device_id=(sp, dp_of[i]), device_id_type=MESH)

    def sp_copy(src, dst, k, sign, s, r):
        return pltpu.make_async_remote_copy(
            src_ref=src, dst_ref=dst, send_sem=s, recv_sem=r,
            device_id=(sp_shifted(me, k, sign), dp), device_id_type=MESH)

    def send_kv(k, c):
        sp_copy(skv.at[k], rkv.at[k], k, 1, kvs_sem, kvr_sem).start()
        return c

    def send_q(k, c):
        sp_copy(sq.at[k], rq.at[k], k, 1, qs_sem, qr_sem.at[k // 2]).start()
        return c

    lax.fori_loop(1, N_SP, send_kv, 0)

    loads[2].wait()
    x_at, core = me[2], me[3]
    right, left, far = lax.rem(x_at + 1, 4), lax.rem(x_at + 3, 4), lax.rem(x_at + 2, 4)
    HALF, SUB = 576, 112
    Y_ROWS, Z_ROWS = 2 * HALF, 2 * HALF + 4 * SUB

    def w_copy(first, size, x_from, device, number):
        at = w.at[pl.ds(first, size), pl.ds(pl.multiple_of((x_from * 2 + core) * 256, 256), 256)]
        return pltpu.make_async_remote_copy(
            src_ref=at, dst_ref=at, send_sem=ws_sem, recv_sem=wr_sem.at[number],
            device_id=device, device_id_type=MESH)

    def w_wait(rows, columns, number):
        at = w.at[pl.ds(0, rows), pl.ds(0, columns)]
        pltpu.make_async_remote_copy(
            src_ref=at, dst_ref=at, send_sem=ws_sem, recv_sem=wr_sem.at[number],
            device_id=(sp, dp), device_id_type=MESH).wait_recv()

    def along_x(x_to):
        return (sp, x_to * 2 + core)

    other_core = (sp, x_at * 2 + 1 - core)
    y_sub = pl.multiple_of(Y_ROWS + me[1] * SUB, 16)
    z_sub = pl.multiple_of(Z_ROWS + me[0] * SUB, 16)
    for x_to in (right, left, far):
        w_copy(y_sub, SUB, x_at, along_x(x_to), 0).start()
        w_copy(z_sub, SUB, x_at, along_x(x_to), 0).start()
    w_copy(0, HALF, x_at, along_x(right), 1).start()
    w_copy(HALF, HALF, x_at, along_x(left), 2).start()
    w_copy(HALF, HALF, x_at, along_x(right), 3).start()
    w_copy(0, HALF, x_at, along_x(left), 4).start()
    w_copy(0, LEN, x_at, other_core, 7).start()
    for c in loads[3:]:
        c.start()

    def y_sub_of(step):
        return pl.multiple_of(Y_ROWS + lax.rem(me[1] + step, 4) * SUB, 16)

    def z_sub_of(step):
        return pl.multiple_of(Z_ROWS + lax.rem(me[0] + step, 4) * SUB, 16)

    def w_lines():
        w_wait(6 * SUB, 256, 0)
        for step in range(1, 4):
            y_to, z_to = lax.rem(me[1] + step, 4), lax.rem(me[0] + step, 4)
            for x_from in (right, left, far):
                w_copy(y_sub, SUB, x_from, (me[0] * 4 + y_to, dp), 16 + step).start()
                w_copy(z_sub, SUB, x_from, (z_to * 4 + me[1], dp), 19 + step).start()
        for x_from in (right, left, far):
            w_copy(y_sub, SUB, x_from, other_core, 5).start()
            w_copy(z_sub, SUB, x_from, other_core, 5).start()

    def w_relay():
        w_wait(HALF, 256, 1)
        w_wait(HALF, 256, 2)
        w_copy(0, HALF, left, along_x(right), 8).start()
        w_copy(HALF, HALF, right, along_x(left), 9).start()
        w_copy(0, HALF, left, other_core, 10).start()
        w_copy(HALF, HALF, right, other_core, 11).start()

    def w_later():
        w_wait(HALF, 256, 3)
        w_wait(HALF, 256, 4)
        w_copy(HALF, HALF, left, other_core, 12).start()
        w_copy(0, HALF, right, other_core, 13).start()

    def w_finish():
        for step in range(1, 4):
            w_wait(3 * SUB, 256, 16 + step)
            for x_from in (right, left, far):
                w_copy(y_sub_of(4 - step), SUB, x_from, other_core, 14).start()
            w_wait(3 * SUB, 256, 19 + step)
            for x_from in (right, left, far):
                w_copy(z_sub_of(4 - step), SUB, x_from, other_core, 14).start()
        w_wait(HALF, 256, 8)
        w_copy(0, HALF, far, other_core, 15).start()
        w_wait(HALF, 256, 9)
        w_copy(HALF, HALF, far, other_core, 16).start()
        w_wait(LEN, 256, 7)
        for number in range(10, 14):
            w_wait(HALF, 256, number)
        w_wait(6 * SUB, 256, 5)
        w_wait(9 * SUB, 512, 14)
        w_wait(HALF, 256, 15)
        w_wait(HALF, 256, 16)

    def w_sent():
        everything = w.at[:, pl.ds(0, 7 * 256)]
        pltpu.make_async_remote_copy(
            src_ref=everything, dst_ref=everything, send_sem=ws_sem, recv_sem=wr_sem.at[0],
            device_id=(sp, dp), device_id_type=MESH).wait_send()

    loads[1].wait()
    prepare_all(q_ref, sq, stacked(cosine * q_gain), stacked(sine * q_turn), False)

    raw = rw_ref[...]
    gates = raw / jnp.sum(raw, axis=0, keepdims=True) * routed_scale
    ids = ids_ref[...]
    hit_t = jnp.zeros((128, 128), jnp.float32)
    gate_t = jnp.zeros((128, 128), jnp.float32)
    for j in range(4):
        on = ids[j : j + 1, :] == row
        hit_t = hit_t + jnp.where(on, 1.0, 0.0)
        gate_t = gate_t + jnp.where(on, gates[j : j + 1, :], 0.0)
    before = (row < lane).astype(jnp.float32).astype(jnp.bfloat16)
    rank_t = jnp.dot(hit_t.astype(jnp.bfloat16), before, preferred_element_type=jnp.float32)
    key_t = jnp.where(hit_t > 0.0, rank_t, -1.0).astype(jnp.bfloat16)
    gate_hi = gate_t.astype(jnp.bfloat16)
    gate_lo = (gate_t - gate_hi.astype(jnp.float32)).astype(jnp.bfloat16)

    table = jnp.concatenate([key_t, gate_hi, gate_lo], axis=1)
    tall_row = lax.broadcasted_iota(jnp.int32, (256, 128), 0)
    tall_lane = lax.broadcasted_iota(jnp.int32, (256, 128), 1)
    for part in range(4):
        d = ((part * 32 + tall_row // SLOT) * STRIDE) & 127
        z = (me[0] + (d >> 5)) & 3
        y = (me[1] + (d >> 3)) & 3
        x = (me[2] + (d >> 1)) & 3
        co = (me[3] + d) & 1
        spread = (z * 32 + y * 8 + x * 2 + co == tall_lane).astype(jnp.float32).astype(jnp.bfloat16)
        found = jnp.dot(spread, table, preferred_element_type=jnp.float32)
        on = found[:, :128] == (tall_row & (SLOT - 1)).astype(jnp.float32)
        at = pl.ds(part * 256, 256)
        pick[at, :] = jnp.where(on, 1.0, 0.0).astype(jnp.bfloat16)
        g_hi[at, :] = jnp.where(on, found[:, 128:256], 0.0).astype(jnp.bfloat16)
        g_lo[at, :] = jnp.where(on, found[:, 256:], 0.0).astype(jnp.bfloat16)

    def clear(i, c):
        ret[pl.ds(pl.multiple_of(i * 16, 16), 16), pl.ds(CAP, SLOT - CAP)] = jnp.zeros((16, SLOT - CAP, 2048), jnp.bfloat16)
        return c

    lax.fori_loop(0, 8, clear, 0)

    for h in range(2):
        wanted = (lax.broadcasted_iota(jnp.int32, (LEN, 128), 1) < 64) == (h == 0)
        vx[pl.ds(h * LEN, LEN), pl.ds(128, 128)] = jnp.where(wanted, 1.0, 0.0).astype(jnp.bfloat16)
    rkv[0] = skv[0]
    rq[0] = sq[0]
    others16 = pl.ds(1, N_SP - 1)

    def sp_all(src, dst, s, r):
        return pltpu.make_async_remote_copy(
            src_ref=src, dst_ref=dst, send_sem=s, recv_sem=r, device_id=(sp, dp), device_id_type=MESH)

    sp_all(skv.at[others16], rkv.at[others16], kvs_sem, kvr_sem).wait_send()
    lax.fori_loop(1, N_SP, send_q, 0)
    sp_all(skv.at[others16], rkv.at[others16], kvs_sem, kvr_sem).wait_recv()

    low_lane = lane < 64

    def lay(g, c):
        for i in range(4):
            k = g * 4 + i
            pair = rkv[k].astype(jnp.float32)
            flipped = jnp.transpose(pair)
            top, none = flipped[0:64], jnp.zeros((64, 128), jnp.float32)
            swapped = pltpu.roll(pair, 64, 1)
            at = pl.ds(pl.multiple_of(k * 128, 128), 128)
            at2 = pl.ds(pl.multiple_of(LEN + k * 128, 128), 128)
            kt[:, at] = jnp.concatenate([top, none], axis=0).astype(jnp.bfloat16)
            kt[:, at2] = jnp.concatenate([none, top], axis=0).astype(jnp.bfloat16)
            vx[at, pl.ds(0, 128)] = jnp.where(low_lane, swapped, 0.0).astype(jnp.bfloat16)
            vx[at2, pl.ds(0, 128)] = jnp.where(low_lane, 0.0, pair).astype(jnp.bfloat16)
        return c

    lax.fori_loop(0, N_SP // 4, lay, 0)
    own_rows = pl.ds(pl.multiple_of(sp * 128, 128), 128)

    def back_rows(k):
        return sp_copy(ao.at[k], rows.at[:, own_rows], k, -1, bs_sem, br_sem)

    def scores(b, target, peaks):
        q = rq[pl.ds(b * 2, 2)].reshape(256, 128)

        def part(at, peak):
            s = jnp.dot(q, kt[:, pl.ds(at, KEYS)], preferred_element_type=jnp.float32)
            target[:, pl.ds(at, KEYS)] = s
            for i in range(0, KEYS, 128):
                peak = s[:, i : i + 128] if peak is None else jnp.maximum(peak, s[:, i : i + 128])
            return peak

        return part

    sp_all(sq.at[1], rq.at[1], qs_sem, qr_sem.at[0]).wait_recv()
    opening = scores(0, s_even, peak_even)
    for h in range(2):
        peak = None
        for at in range(h * LEN, h * LEN + LEN, KEYS):
            peak = opening(at, peak)
        peak_even[:, pl.ds(h * 128, 128)] = peak

    def block(b, held, held_peak, following, following_peak):
        @pl.when(b < BLOCKS - 1)
        def _():
            two = pl.ds(b * 2 + 2, 2)
            sp_all(sq.at[two], rq.at[two], qs_sem, qr_sem.at[b + 1]).wait_recv()

        part = scores(jnp.minimum(b + 1, BLOCKS - 1), following, following_peak)
        o = None
        for h in range(2):
            top = jnp.max(held_peak[:, pl.ds(h * 128, 128)], axis=1, keepdims=True)
            peak = None
            for at in range(h * LEN, h * LEN + LEN, KEYS):
                peak = part(at, peak)
                p = jnp.exp2((held[:, pl.ds(at, KEYS)] - top) * EXP_SCALE).astype(jnp.bfloat16)
                d = jnp.dot(p, vx[pl.ds(at, KEYS), :], preferred_element_type=jnp.float32)
                o = d if o is None else o + d
            following_peak[:, pl.ds(h * 128, 128)] = peak
        a = (o[:, :128] / o[:, 128:]).astype(jnp.bfloat16)
        ao[pl.ds(b * 2, 2)] = a.reshape(2, 128, 128)

        @pl.when(b > 0)
        def _():
            back_rows(b * 2).start()

        back_rows(b * 2 + 1).start()

    def two_blocks(i, c):
        block(i * 2, s_even, peak_even, s_odd, peak_odd)
        @pl.when(i == 0)
        def _():
            w_lines()

        block(i * 2 + 1, s_odd, peak_odd, s_even, peak_even)

        @pl.when(i == 1)
        def _():
            w_relay()

        @pl.when(i == 2)
        def _():
            w_later()

        return c

    lax.fori_loop(0, BLOCKS // 2, two_blocks, 0)
    rows[:, own_rows] = ao[0]
    sp_all(sq.at[others16], rq.at[others16], qs_sem, qr_sem.at[0]).wait_send()
    w_finish()
    back_all16 = sp_all(ao.at[others16], ao.at[others16], bs_sem, br_sem)
    back_all16.wait_send()
    back_all16.wait_recv()

    loads[3].wait()
    total = jnp.zeros((128, 1), jnp.float32)
    for n in range(4):
        cols = pl.ds(n * 512, 512)
        part = jnp.dot(rows[...], w[:, cols], preferred_element_type=jnp.float32)
        part = part + res_ref[:, cols].astype(jnp.float32)
        mixed[:, cols] = part
        total = total + jnp.sum(part * part, axis=1, keepdims=True)
    scale = lax.rsqrt(total / 2048.0 + norm_eps)
    normed[...] = (mixed[...] * scale * ngain_ref[...]).astype(jnp.bfloat16)

    pl.semaphore_wait(all_sem, 7)

    def send_copy(k):
        return pltpu.make_async_remote_copy(
            src_ref=send.at[k, pl.ds(0, CAP)], dst_ref=recv.at[k, pl.ds(0, CAP)],
            send_sem=s_sem, recv_sem=r_sem.at[k // PER],
            device_id=shifted(me, k, 1), device_id_type=MESH)

    def send_block(first, count, sem):
        at = pl.ds(first, count)
        return pltpu.make_async_remote_copy(
            src_ref=send.at[at, pl.ds(0, CAP)], dst_ref=recv.at[at, pl.ds(0, CAP)],
            send_sem=s_sem, recv_sem=sem, device_id=(sp, dp), device_id_type=MESH)

    def pack(chunk, c):
        at = pl.ds(pl.multiple_of(chunk * 128, 128), 128)
        packed = jnp.dot(pick[at, :], normed[...], preferred_element_type=jnp.float32).astype(jnp.bfloat16)
        send[pl.ds(pl.multiple_of(chunk * 16, 16), 16)] = packed.reshape(16, SLOT, 2048)

        def start(i, c):
            send_copy((chunk - 1) * 16 + i).start()
            return c

        lax.fori_loop(jnp.where(chunk == 1, 1, 0), jnp.where(chunk == 0, 0, 16), start, 0)
        return c

    lax.fori_loop(0, 8, pack, 0)
    lax.fori_loop(112, 128, lambda k, c: (send_copy(k).start(), c)[1], 0)
    recv[0] = send[0]

    for c in loads[4:7]:
        c.wait()
    xs = normed[...]
    hidden = silu_mul(
        jnp.dot(xs, sg[...], preferred_element_type=jnp.float32),
        jnp.dot(xs, su[...], preferred_element_type=jnp.float32)).astype(jnp.bfloat16)
    for n in range(4):
        cols = pl.ds(n * 512, 512)
        mixed[:, cols] = mixed[:, cols] + jnp.dot(hidden, sd[:, cols], preferred_element_type=jnp.float32)

    for c in loads[7:]:
        c.wait()

    def back_copy(k):
        return pltpu.make_async_remote_copy(
            src_ref=fout.at[k, pl.ds(0, CAP)], dst_ref=ret.at[k, pl.ds(0, CAP)],
            send_sem=s2_sem, recv_sem=r2_sem.at[k // PER],
            device_id=shifted(me, k, -1), device_id_type=MESH)

    def expert(g, c):
        first = g * PER
        lo = jnp.where(g == 0, 1, 0)

        @pl.when(g == 0)
        def _():
            send_block(1, PER - 1, r_sem.at[0]).wait_recv()

        @pl.when(g > 0)
        def _():
            send_block(pl.multiple_of(first, PER), PER, r_sem.at[g]).wait_recv()

        at = pl.ds(pl.multiple_of(first, PER), PER)
        x = recv[at].reshape(PER * SLOT, 2048)
        hid[...] = silu_mul(
            jnp.dot(x, eg[...], preferred_element_type=jnp.float32),
            jnp.dot(x, eu[...], preferred_element_type=jnp.float32)).astype(jnp.bfloat16)
        h = hid[...]
        for n in range(4):
            cols = pl.ds(n * 512, 512)
            o = jnp.dot(h, ed[:, cols], preferred_element_type=jnp.float32).astype(jnp.bfloat16)
            fout[at, :, cols] = o.reshape(PER, SLOT, 512)

        def reply(i, c):
            back_copy(first + i).start()
            return c

        lax.fori_loop(lo, PER, reply, 0)
        return c

    lax.fori_loop(0, GROUPS, expert, 0)

    ret[0, pl.ds(0, CAP)] = fout[0, pl.ds(0, CAP)]

    def back_block(first, count, number):
        at = pl.ds(first, count)
        return pltpu.make_async_remote_copy(
            src_ref=fout.at[at, pl.ds(0, CAP)], dst_ref=ret.at[at, pl.ds(0, CAP)],
            send_sem=s2_sem, recv_sem=r2_sem.at[number], device_id=(sp, dp), device_id_type=MESH)

    w_sent()
    send_block(1, N_DEV - 1, r_sem.at[0]).wait_send()
    dims = (((0,), (0,)), ((), ()))
    for g in range(GROUPS):
        first = max(1, g * PER)
        back_block(first, (g + 1) * PER - first, g).wait_recv()
        at = pl.ds(g * PER * SLOT, PER * SLOT)
        for n in range(4):
            cols = pl.ds(n * 512, 512)
            r = ret[pl.ds(g * PER, PER), :, cols].reshape(PER * SLOT, 512)
            routed = lax.dot_general(g_hi[at, :], r, dims, preferred_element_type=jnp.float32)
            routed = routed + lax.dot_general(g_lo[at, :], r, dims, preferred_element_type=jnp.float32)
            if g < GROUPS - 1:
                mixed[:, cols] = mixed[:, cols] + routed
            else:
                out_ref[:, cols] = (mixed[:, cols] + routed).astype(jnp.bfloat16)
    back_block(1, N_DEV - 1, 0).wait_send()


def layer(*operands):
    bf, f32 = jnp.bfloat16, jnp.float32
    V, A = pl.BlockSpec(memory_space=pltpu.VMEM), pl.BlockSpec(memory_space=pl.ANY)
    S = pltpu.SemaphoreType.DMA
    M = pltpu.VMEM
    return pl.pallas_call(
        layer_kernel,
        out_shape=pltpu.VMEM((128, 2048), bf),
        in_specs=[A, A, V, V, V, V, A, A, V, V, V, A, A, A, A, A, A],
        out_specs=V,
        scratch_shapes=[
            M((128, 16, 128), bf), M((128, 16, 128), bf), M((128, 2048), bf),
            M((2048, 2048), bf),
            M((2048, 512), bf), M((2048, 512), bf), M((512, 2048), bf),
            M((2048, 512), bf), M((2048, 512), bf), M((512, 2048), bf),
            M((128, 2048), f32), M((128, 2048), bf),
            M((1024, 128), bf), M((1024, 128), bf), M((1024, 128), bf),
            M((128, SLOT, 2048), bf), M((128, SLOT, 2048), bf),
            M((128, SLOT, 2048), bf), M((128, SLOT, 2048), bf),
            M((PER * SLOT, 512), bf),
            M((LEN, 128), f32), M((N_SP, 128, 128), bf), M((N_SP, 128, 128), bf), M((N_SP, 128, 128), bf),
            M((N_SP, 128, 128), bf), M((128, 2 * LEN), bf), M((2 * LEN, 256), bf), M((N_SP, 128, 128), bf),
            M((128, 2048), bf), M((256, 2 * LEN), f32), M((256, 2 * LEN), f32), M((256, 256), f32), M((256, 256), f32),
            S((10,)), S, S((GROUPS,)), S, S((GROUPS,)), S, S, S, S((BLOCKS,)), S, S, S, S((23,)), pltpu.SemaphoreType.REGULAR,
        ],
        compiler_params=pltpu.CompilerParams(collective_id=0, has_side_effects=True, vmem_limit_bytes=63 * 2**20),
        name="layer",
    )(*operands)


def per_device(
    residual, query, key_value, out_weight, norm_gain, query_gain, key_gain, route_ids, route_weights,
    shared_gate, shared_up, shared_down, expert_gate, expert_up, expert_down,
):
    cosine, sine = rope_tables()
    combined = layer(
        query[0], key_value[0], jnp.asarray(cosine), jnp.asarray(sine), query_gain[None, :], key_gain[None, :],
        out_weight, residual[0], norm_gain[None, :], route_ids[0].T, route_weights[0].T,
        shared_gate, shared_up, shared_down, expert_gate, expert_up, expert_down,
    )
    return combined[None]


def solution(mesh):
    in_specs = (
        P("dp", "sp", None),
        P("dp", "sp", None, None),
        P("dp", "sp", None, None),
        P(None, "dp"),
        P(),
        P(),
        P(),
        P("dp", "sp", None),
        P("dp", "sp", None),
        P(),
        P(),
        P(),
        P(("sp", "dp"), None, None),
        P(("sp", "dp"), None, None),
        P(("sp", "dp"), None, None),
    )
    out_specs = P("dp", "sp", None)
    return jax.shard_map(
        per_device, mesh=mesh, in_specs=in_specs, out_specs=out_specs, check_vma=False
    )
```
